256 devices in a mesh: ep: 64 (over z, x, core), tp: 4 (over y).
Axes of the slice: x: 4, y: 4, z: 8, core: 2. Of those that a mesh axis runs over, the one named last changes fastest.
Arguments:
- query_rows: bfloat16 [8192, 1024], P('ep', 'tp'), may hold values from -6 to 6
- key_rows: bfloat16 [8192, 256], P('ep', 'tp'), may hold values from -6 to 6
- retrieved_vector_table: bfloat16 [8192, 256], P('ep', 'tp'), may hold values from -6 to 6
- key_bias: bfloat16 [8192, 4], P('ep', 'tp'), may hold values from -1.5 to 12
- score_offset: float32 [16], P('tp'), may hold values from 3 to 12
- out_weight: bfloat16 [1024, 2048], P('tp'), may hold values from -0.1875 to 0.1875
- second_batch_activations: bfloat16 [8192, 2048], P('ep'), may hold values from -6 to 6
- norm_gain: float32 [2048], replicated, may hold values from 0.1 to 1.9
- expert_index: int32 [8192, 2], P('ep'), may hold values from 0 to 63, all different within a row; in each aligned block of 128 rows (0 to 127, 128 to 255, ...) at most 8 rows name the same one
- route_weight: float32 [8192, 2], P('ep'), may hold values from 0.2 to 1
- gate_weight: bfloat16 [64, 2048, 1024], P('ep', None, 'tp'), may hold values from -0.125 to 0.125
- up_weight: bfloat16 [64, 2048, 1024], P('ep', None, 'tp'), may hold values from -0.125 to 0.125
- down_weight: bfloat16 [64, 1024, 2048], P('ep', 'tp'), may hold values from -0.1875 to 0.1875
Outputs:
- attention_out: bfloat16 [8192, 2048], P(('ep', 'tp'))
- expert_out: bfloat16 [8192, 2048], P('ep', 'tp')
The draws below stay inside these ranges and needn't reach their ends.
Inputs may be any that keep to these rules, and one draw needn't show every extreme that they name: `expert_index`: each row names 2 different experts; in each aligned block of 128 rows (the rows of one index of ep) no expert is named by more than 8 rows, a bound that some block reaches.
All inputs are finite; a program needn't handle non-finite values.
Results may differ from the reference program's by a relative error of at most 0.011.
Values may be sent and summed in bfloat16 or wider, within the bound.
A program may use at most 64 MiB of HBM per device.

```python
import math
import jax
import jax.numpy as jnp
import numpy as np
from jax import lax

D = 2048
HEADS = 16
KVH = 4
HD = 64
FF = 1024
TOP = 2
SEQS = 1
ROWS_A = 128
TOK_B = 128
EXPERTS = 64
CAP = 8
LENGTH = 8192
TOKENS_A = 8192
TOKENS_B = 8192
N_EP = 64
N_TP = 4


def draw_score_offset(key, part):
    slow_key, fast_key, pick_key = jax.random.split(jax.random.fold_in(key, 11), 3)
    base = max(math.log(LENGTH) - 0.5, 3.5)
    slow = base + jax.random.uniform(slow_key, (HEADS,), jnp.float32, 0.0, 1.0)
    fast = 3.0 + jax.random.uniform(fast_key, (HEADS,), jnp.float32, 0.0, 0.8)
    share = 0.5
    slow_heads = jax.random.uniform(pick_key, (HEADS,), jnp.float32) < share
    return jnp.where(slow_heads, slow, fast).astype(jnp.float32)


def draw_key_bias(key, part):
    block_key, spot_key, size_key = jax.random.split(jax.random.fold_in(key, 23), 3)
    blocks = TOKENS_A // ROWS_A
    reach = 1.0
    block_level = jax.random.uniform(block_key, (blocks, 1, KVH), jnp.float32, -reach, reach)
    block_level = jnp.broadcast_to(block_level, (blocks, ROWS_A, KVH)).reshape(TOKENS_A, KVH)
    spots = jax.random.randint(spot_key, (SEQS, 3), 0, LENGTH)
    starts = jnp.arange(SEQS, dtype=jnp.int32)[:, None] * LENGTH
    flagged_entries = (starts + spots).reshape(-1)
    position_index = jnp.arange(TOKENS_A, dtype=jnp.int32)
    flagged_rows = jnp.any(position_index[:, None] == flagged_entries[None, :], axis=1)
    spot_logit = math.log(LENGTH) + jax.random.uniform(size_key, (TOKENS_A, KVH), jnp.float32, -1.0, 0.5)
    return jnp.where(flagged_rows[:, None], spot_logit, block_level).astype(jnp.bfloat16)


def block_scale(key, shape, shards, smallest, top_value):
    level, own = 1.0, jax.random.fold_in(key, 6)
    for dim, blocks in shards:
        steps = jnp.exp(jax.random.uniform(jax.random.fold_in(own, dim), (blocks,), jnp.float32, smallest / len(shards), top_value / len(shards)))
        level = level * jnp.repeat(steps, shape[dim] // blocks).reshape([-1 if axis == dim else 1 for axis in range(len(shape))])
    return level


def routed_block(own_key, own, number, rows, amount, top, most, skew):
    ranking = jax.random.permutation(own_key, amount)
    packed, usual = portions_of(amount, rows * top, most, skew, True), portions_of(amount, rows * top, most, skew, False)
    places = jnp.arange(amount)

    def named(tallies, rotation):
        used = int((tallies > 0).sum())
        fixed = max(1, used // 4)
        shifted = fixed + (places - fixed + rotation * (used - fixed)) % max(1, amount - fixed)
        return jnp.zeros((amount,), jnp.int32).at[ranking[jnp.where(places < fixed, places, shifted)]].set(jnp.asarray(tallies, jnp.int32))

    tallies = jnp.where(number % 4 == 0, named(packed, number // 4), named(usual, number - number // 4 - 1))
    mixed = jax.random.permutation(jax.random.fold_in(own, 3), amount)
    source_of, receiver = mixed[0:amount // 2 * 2:2], mixed[1:amount // 2 * 2:2]
    room = jnp.minimum(tallies[source_of] - 1, most - tallies[receiver]) // 2
    room = jnp.where((source_of == ranking[0]) | (receiver == ranking[0]) | (tallies[receiver] == 0), 0, jnp.maximum(room, 0))
    shifted = jax.random.randint(jax.random.fold_in(own, 4), (amount // 2,), 0, 1 << 20) % (room + 1)
    tallies = tallies.at[source_of].add(-shifted).at[receiver].add(shifted)
    items = jnp.searchsorted(jnp.cumsum(tallies), jnp.arange(rows * top), side="right").astype(jnp.int32)
    listing = items.reshape(top, rows).T
    listing = listing[jax.random.permutation(jax.random.fold_in(own, 1), rows)]
    rotation = jax.random.randint(jax.random.fold_in(own, 2), (rows, 1), 0, top)
    return jnp.take_along_axis(listing, (jnp.arange(top)[None, :] + rotation) % top, axis=1)


def portions_of(number_of, total, bound, skew, full):
    loads = [(1 << 20) // math.isqrt(standing ** skew) + 1 for standing in range(1, number_of + 1)]
    largest = bound if full else min(bound, max(-(-total // number_of), total * loads[0] // sum(loads)))
    least = 1 if total - largest >= number_of - 1 else 0
    holding, spare = [largest] + [least] * (number_of - 1), total - largest - least * (number_of - 1)
    while spare > 0:
        free = [i for i in range(1, number_of) if holding[i] < largest] or [i for i in range(1, number_of) if holding[i] < bound]
        whole, budget = sum([loads[i] for i in free]), spare
        for i in free:
            extra = min(bound - holding[i], max(1, budget * loads[i] // whole), spare)
            holding[i] = holding[i] + extra
            spare = spare - extra
    return np.array(holding)


def centred(own_key, extent, scale, most, cuts=(), kind=jnp.bfloat16):
    values = scale * jax.random.normal(own_key, extent, jnp.float32)
    if cuts:
        values = values * block_scale(own_key, extent, cuts, -0.22, 0.18)
    return jnp.clip(values, -most, most).astype(kind)


def setup_inputs(seed: int = 0) -> dict:
    key_of = jax.random.split(jax.random.key(seed), 14)
    query_rows = centred(key_of[0], (TOKENS_A, HEADS * HD), 1.0, 6.0, ((0, 64), (1, 4)))
    key_rows = centred(key_of[1], (TOKENS_A, KVH * HD), 1.0, 6.0, ((0, 64), (1, 4)))
    retrieved_vector_table = centred(key_of[2], (TOKENS_A, KVH * HD), 1.0, 6.0, ((0, 64), (1, 4)))
    key_bias = draw_key_bias(jax.random.fold_in(key_of[13], 71), 0)
    score_offset = draw_score_offset(jax.random.fold_in(key_of[13], 71), 0)
    out_weight = centred(key_of[5], (HEADS * HD, D), (HEADS * HD) ** -0.5, 0.1875, ((0, 4),))
    second_batch_activations = centred(key_of[6], (TOKENS_B, D), 1.0, 6.0, ((0, 64),))
    norm_gain = jnp.clip(1.0 + 0.18 * jax.random.normal(key_of[7], (D,), jnp.float32), 0.1, 1.9)
    expert_index_keys = jax.random.split(jax.random.fold_in(key_of[8], 1), TOKENS_B // TOK_B)
    expert_index_turns = jax.random.permutation(jax.random.fold_in(key_of[8], 3), TOKENS_B // TOK_B)
    expert_index = jax.vmap(lambda own, number: routed_block(jax.random.fold_in(key_of[8], 2), own, number, TOK_B, EXPERTS, TOP, CAP, 2))(expert_index_keys, expert_index_turns).reshape((TOKENS_B, TOP))
    route_weight = jnp.clip(0.2 + 0.8 * jax.random.uniform(key_of[9], (TOKENS_B, TOP), jnp.float32) ** block_scale(key_of[9], (TOKENS_B, TOP), ((0, 64),), -0.2, 0.2), 0.2, 1.0)
    gate_weight = centred(key_of[10], (EXPERTS, D, FF), D ** -0.5, 0.125, ((0, 64), (2, 4)))
    up_weight = centred(key_of[11], (EXPERTS, D, FF), D ** -0.5, 0.125, ((0, 64), (2, 4)))
    down_weight = centred(key_of[12], (EXPERTS, FF, D), FF ** -0.5, 0.1875, ((0, 64), (1, 4)))
    return dict(query_rows=query_rows, key_rows=key_rows, retrieved_vector_table=retrieved_vector_table, key_bias=key_bias, score_offset=score_offset, out_weight=out_weight, second_batch_activations=second_batch_activations, norm_gain=norm_gain, expert_index=expert_index, route_weight=route_weight, gate_weight=gate_weight, up_weight=up_weight, down_weight=down_weight)


def block_terms(query_block, key_block, value_block, bias_block, offset, causal_mask):
    scale = 1.0 / math.sqrt(query_block.shape[-1])
    scores = jnp.einsum('tkgd,skd->kgts', query_block.astype(jnp.float32), key_block.astype(jnp.float32)) * scale
    scores = scores + jnp.transpose(bias_block.astype(jnp.float32))[:, None, None, :] - offset[:, :, None, None]
    length = query_block.shape[0]
    if causal_mask:
        later = lax.broadcasted_iota(jnp.int32, (length, length), 0) > lax.broadcasted_iota(jnp.int32, (length, length), 1)
        keep = jnp.where(later, jax.nn.log_sigmoid(-scores), 0.0)
        suffix = lax.cumsum(keep, axis=3, reverse=True) - keep
        weight = jnp.where(later, jnp.exp(jax.nn.log_sigmoid(scores) + suffix), 0.0)
    else:
        keep = jax.nn.log_sigmoid(-scores)
        suffix = lax.cumsum(keep, axis=3, reverse=True) - keep
        weight = jnp.exp(jax.nn.log_sigmoid(scores) + suffix)
    weight = weight.astype(jnp.bfloat16)
    block_out = jnp.einsum('kgts,skd->kgtd', weight.astype(jnp.float32), value_block.astype(jnp.float32))
    return (block_out, lax.optimization_barrier(jnp.sum(keep, axis=3)))

def attention_half(query_rows, key_rows, retrieved_vector_table, key_bias, score_offset, out_weight):
    group = HEADS // KVH
    span = N_EP // SEQS
    blocks = query_rows.shape[0] // ROWS_A
    queries = query_rows.reshape(blocks, ROWS_A, KVH, group, HD)
    keyset = key_rows.reshape(blocks, ROWS_A, KVH, HD)
    valueset = retrieved_vector_table.reshape(blocks, ROWS_A, KVH, HD)
    biases = key_bias.reshape(blocks, ROWS_A, KVH)
    offset = score_offset.reshape(KVH, group)

    def one_block(block_index):
        query_block = queries[block_index]
        result, near = block_terms(query_block, keyset[block_index], valueset[block_index], biases[block_index], offset, True)
        first = block_index - block_index % span

        def step(distance, state):
            result, near = state
            source = block_index - distance
            block_out, total = block_terms(query_block, keyset[source], valueset[source], biases[source], offset, False)
            return (result + jnp.exp(near)[..., None] * block_out, near + total)
        result, near = lax.fori_loop(1, block_index - first + 1, step, (result, near))
        return result
    outs = lax.map(one_block, jnp.arange(blocks, dtype=jnp.int32))
    attended = jnp.transpose(outs, (0, 3, 1, 2, 4)).reshape(query_rows.shape[0], HEADS * HD).astype(jnp.bfloat16)
    width = attended.shape[1] // N_TP
    summed = jnp.zeros((attended.shape[0], out_weight.shape[1]), jnp.float32)
    for section in range(N_TP):
        product_terms = jnp.dot(attended[:, section * width:(section + 1) * width], out_weight[section * width:(section + 1) * width], preferred_element_type=jnp.float32)
        rounded = lax.optimization_barrier(product_terms.astype(jnp.bfloat16))
        summed = summed + rounded.astype(jnp.float32)
    return summed.astype(jnp.bfloat16)

def expert_half(second_batch_activations, norm_gain, expert_index, route_weight, gate_weight, up_weight, down_weight):
    values32 = second_batch_activations.astype(jnp.float32)
    normed = (values32 * lax.rsqrt(lax.optimization_barrier(jnp.mean(values32 * values32, axis=1, keepdims=True)) + 1e-06) * norm_gain).astype(jnp.bfloat16)
    flat = expert_index.reshape(-1)
    weights = route_weight.reshape(-1)
    limit = N_EP * CAP
    width = FF // N_TP

    def one_expert(summed, expert):
        chosen = jnp.nonzero(flat == expert, size=limit, fill_value=0)[0].astype(jnp.int32)
        count = jnp.sum((flat == expert).astype(jnp.int32))
        valid = jnp.arange(limit, dtype=jnp.int32) < count
        token = chosen // TOP
        rows = normed[token]
        gate_pre = jnp.dot(rows, gate_weight[expert], preferred_element_type=jnp.float32)
        up_pre = jnp.dot(rows, up_weight[expert], preferred_element_type=jnp.float32)
        hidden = (jax.nn.silu(gate_pre) * up_pre).astype(jnp.bfloat16)
        down = down_weight[expert]
        result = jnp.zeros((limit, D), jnp.float32)
        for section in range(N_TP):
            product_terms = jnp.dot(hidden[:, section * width:(section + 1) * width], down[section * width:(section + 1) * width], preferred_element_type=jnp.float32)
            rounded = lax.optimization_barrier(product_terms.astype(jnp.bfloat16))
            result = result + rounded.astype(jnp.float32)
        result = result.astype(jnp.bfloat16).astype(jnp.float32)
        scale = jnp.where(valid, weights[chosen], 0.0)
        return (summed.at[token].add(scale[:, None] * result), None)
    summed, unused = lax.scan(one_expert, jnp.zeros((second_batch_activations.shape[0], D), jnp.float32), jnp.arange(EXPERTS, dtype=jnp.int32))
    return summed.astype(jnp.bfloat16)

def reference(query_rows, key_rows, retrieved_vector_table, key_bias, score_offset, out_weight, second_batch_activations, norm_gain, expert_index, route_weight, gate_weight, up_weight, down_weight):
    attention_out = attention_half(query_rows, key_rows, retrieved_vector_table, key_bias, score_offset, out_weight)
    expert_out = expert_half(second_batch_activations, norm_gain, expert_index, route_weight, gate_weight, up_weight, down_weight)
    return (attention_out, expert_out)
```

```python
import jax
import jax.numpy as jnp
from jax import lax
from jax.experimental import pallas as pl
from jax.experimental.pallas import tpu as pltpu
from jax.sharding import PartitionSpec as P

HD = 64
LOG2E = 1.4426950408889634
ROWS = 128


def block_update(lhs, off, kv, bias_row, tri, near, diag):
    rhs = jnp.concatenate([kv, kv], axis=1)
    dot = lax.dot_general(lhs, rhs, (((1,), (1,)), ((), ())), preferred_element_type=jnp.float32)
    heads = dot.shape[0] // ROWS
    s = jnp.concatenate(
        [dot[h * ROWS : (h + 1) * ROWS] + (bias_row - off[h]) for h in range(heads)], axis=0
    )
    small = jnp.log2(1.0 + jnp.exp2(-jnp.abs(s)))
    soft = jnp.maximum(s, 0.0) + small
    logw = jnp.minimum(s, 0.0) - small
    if diag:
        row = lax.broadcasted_iota(jnp.int32, s.shape, 0) % ROWS
        later = row > lax.broadcasted_iota(jnp.int32, s.shape, 1)
        soft = jnp.where(later, soft, 0.0)
    sums = jnp.dot(soft.astype(jnp.bfloat16), tri, preferred_element_type=jnp.float32)
    expo = logw - sums[:, :ROWS]
    if near is not None:
        expo = expo - near
    w = jnp.exp2(expo)
    if diag:
        w = jnp.where(later, w, 0.0)
    out = jnp.dot(w.astype(jnp.bfloat16), kv, preferred_element_type=jnp.float32)
    return out, sums[:, ROWS:]


def query_lhs(q):
    q2 = q.astype(jnp.float32) * (0.125 * LOG2E)
    hi = q2.astype(jnp.bfloat16)
    lo = (q2 - hi.astype(jnp.float32)).astype(jnp.bfloat16)
    zero = jnp.zeros((ROWS, HD), jnp.bfloat16)
    parts = []
    for h in range(q.shape[1] // HD):
        cut = slice(h * HD, (h + 1) * HD)
        parts.append(jnp.concatenate([hi[:, cut], zero, lo[:, cut], zero], axis=1))
    return jnp.concatenate(parts, axis=0)


def triangle():
    r = lax.broadcasted_iota(jnp.int32, (ROWS, 2 * ROWS), 0)
    c = lax.broadcasted_iota(jnp.int32, (ROWS, 2 * ROWS), 1)
    return jnp.where((r > c) | (c >= ROWS), 1.0, 0.0).astype(jnp.bfloat16)


NX, NC, CAP = 4, 2, 8
DISTANCES = ((0, 1), (7, 2), (6, 3), (5, 4))
MESH = pl.DeviceIdType.MESH


def whole_kernel(
    off_ref, pack_ref, q_ref, act_ref, gain_ref, idx_ref, idxt_ref, route_ref, wg_hbm, wu_hbm, wd_hbm, wo_hbm,
    att_out, exp_out,
    kvb, lhs_ref, tri_ref, acc_ref, near_ref,
    wg, wu, wd, wo,
    outgoing, pick, arr, part, rs1l, rs1r, rs2l, rs2r, res, ret,
    apart, ars1l, ars1r, ars2l, ars2r,
    wsem, lsem, kzs, kzr, kxs, kxr, kcs, kcr, ds, dr, ags, agr, rss, rsr, rts, rtr, ats, atr,
):
    e, t = lax.axis_index("ep"), lax.axis_index("tp")
    nz = lax.axis_size("ep") // (NX * NC)
    ne = nz * NX * NC
    tokens = act_ref.shape[0]
    heads = q_ref.shape[1] // HD
    groups = arr.shape[1]
    wide = arr.shape[-1]
    z, x, c = e // (NX * NC), e // NC % NX, e % NC
    xc = x * NC + c
    left, right, opp = (t + 3) % 4, (t + 1) % 4, (t + 2) % 4

    def ep_of(z_, x_, c_):
        return (z_ * NX + x_) * NC + c_

    def rc(src, dst, ssem, rsem, dev):
        return pltpu.make_async_remote_copy(
            src_ref=src, dst_ref=dst, send_sem=ssem, recv_sem=rsem, device_id=dev, device_id_type=MESH
        )

    barrier = pltpu.get_barrier_semaphore()

    def greet(i, carry):
        pl.semaphore_signal(barrier, inc=1, device_id=((e + i) % ne, t), device_id_type=MESH)
        return carry

    lax.fori_loop(1, ne, greet, 0)
    for near_t in (left, right):
        pl.semaphore_signal(barrier, inc=1, device_id=(e, near_t), device_id_type=MESH)

    loads = [
        pltpu.make_async_copy(src, dst, wsem.at[i])
        for i, (src, dst) in enumerate(((wg_hbm, wg), (wu_hbm, wu), (wd_hbm, wd), (wo_hbm, wo)))
    ]
    for load in loads:
        load.start()
    own_kv = pltpu.make_async_copy(pack_ref, kvb.at[xc, z], lsem.at[0])
    own_kv.start()

    values = act_ref[...].astype(jnp.float32)
    inv = lax.rsqrt(jnp.mean(values * values, axis=1, keepdims=True) + 1e-06)
    mine = pl.ds(pl.multiple_of(t * wide, wide), wide)
    normed = (act_ref[:, mine].astype(jnp.float32) * inv * gain_ref[:, mine]).astype(jnp.bfloat16)
    i0 = lax.broadcasted_iota(jnp.int32, (tokens, tokens), 0)
    i1 = lax.broadcasted_iota(jnp.int32, (tokens, tokens), 1)
    below = jnp.where(i0 > i1, 1.0, 0.0).astype(jnp.bfloat16)
    above = jnp.where(i0 < i1, 1.0, 0.0).astype(jnp.bfloat16)
    eq = [jnp.where(i1 == idx_ref[:, k : k + 1], 1.0, 0.0) for k in range(2)]
    prefix = jnp.dot(below, (eq[0] + eq[1]).astype(jnp.bfloat16), preferred_element_type=jnp.float32)
    eqt = [jnp.where(i0 == idxt_ref[k : k + 1, :], 1.0, 0.0) for k in range(2)]
    prefixt = jnp.dot((eqt[0] + eqt[1]).astype(jnp.bfloat16), above, preferred_element_type=jnp.float32)
    slots = ne * CAP
    col = lax.broadcasted_iota(jnp.int32, (tokens, slots), 1).astype(jnp.float32)
    row = lax.broadcasted_iota(jnp.int32, (slots, tokens), 0).astype(jnp.float32)
    spread = None
    for k in range(2):
        place = jnp.sum(eq[k] * prefix, axis=1, keepdims=True) + idx_ref[:, k : k + 1].astype(jnp.float32) * CAP
        pick[k] = jnp.where(col == place, 1.0, 0.0).astype(jnp.bfloat16)
        placet = jnp.sum(eqt[k] * prefixt, axis=0, keepdims=True) + idxt_ref[k : k + 1, :].astype(jnp.float32) * CAP
        one = jnp.where(row == placet, 1.0, 0.0)
        spread = one if spread is None else spread + one
    sent = jnp.dot(spread.astype(jnp.bfloat16), normed, preferred_element_type=jnp.float32)
    outgoing[...] = sent.reshape(ne, CAP, wide).astype(jnp.bfloat16)
    lhs_ref[...] = query_lhs(q_ref[...])
    tri_ref[...] = triangle()
    off = [off_ref[h] * LOG2E for h in range(heads)]

    pl.semaphore_wait(barrier, ne + 1)

    def to_z(i, carry):
        rc(pack_ref, kvb.at[xc, z], kzs, kzr, (ep_of((z + i) % nz, x, c), t)).start()
        return carry

    lax.fori_loop(1, nz, to_z, 0)

    def peer(g, i, sign):
        per = NX * NC
        dz = jnp.where(i < per, DISTANCES[g][0] % nz, DISTANCES[g][1] % nz)
        dx, dc = i // NC % NX, i % NC
        if sign < 0:
            dz, dx = nz - dz, NX - dx
        return ep_of((z + dz) % nz, (x + dx) % NX, (c + dc) % NC)

    own_rows = pltpu.make_async_copy(outgoing.at[e], arr.at[t, 0, 0], lsem.at[1])
    own_rows.start()
    for g in range(groups):

        def scatter(i, carry, g=g):
            to = peer(g, i, 1)
            rc(outgoing.at[to], arr.at[t, g, i], ds.at[g], dr.at[g], (to, t)).start()
            return carry

        lax.fori_loop(1 if g == 0 else 0, 2 * NX * NC, scatter, 0)

    def arrived(g):
        ref = arr.at[t, g, 1:] if g == 0 else arr.at[t, g]
        return rc(ref, ref, ds.at[g], dr.at[g], (e, t))

    half = arr.shape[2] // 2
    at_right, at_left = (e, right), (e, left)

    def ag(g):
        return [
            rc(arr.at[t, g], arr.at[t, g], ags.at[0, g], agr.at[0, g], at_right),
            rc(arr.at[t, g], arr.at[t, g], ags.at[1, g], agr.at[1, g], at_left),
            rc(arr.at[left, g, :half], arr.at[left, g, :half], ags.at[2, g], agr.at[2, g], at_right),
            rc(arr.at[right, g, half:], arr.at[right, g, half:], ags.at[3, g], agr.at[3, g], at_left),
        ]

    ags_all = [ag(g) for g in range(groups)]

    def spread_rows(g):
        arrived(g).wait_recv()
        if g == 0:
            own_rows.wait()
        ags_all[g][0].start()
        ags_all[g][1].start()

    def forward_rows(g):
        ags_all[g][0].wait_recv()
        ags_all[g][2].start()
        ags_all[g][1].wait_recv()
        ags_all[g][3].start()

    xl, xr, xo = (x + 3) % NX, (x + 1) % NX, (x + 2) % NX
    dev_xr, dev_xl, dev_c = (ep_of(z, xr, c), t), (ep_of(z, xl, c), t), (ep_of(z, x, (c + 1) % NC), t)
    zh = nz // 2

    def grp(x_):
        return kvb.at[x_ * NC + c]

    kx = [
        rc(grp(x), grp(x), kxs.at[0], kxr.at[0], dev_xr),
        rc(grp(x), grp(x), kxs.at[1], kxr.at[1], dev_xl),
        rc(kvb.at[xl * NC + c, :zh], kvb.at[xl * NC + c, :zh], kxs.at[2], kxr.at[2], dev_xr),
        rc(kvb.at[xr * NC + c, zh:], kvb.at[xr * NC + c, zh:], kxs.at[3], kxr.at[3], dev_xl),
    ]
    kc = [rc(grp(x_), grp(x_), kcs.at[i], kcr.at[i], dev_c) for i, x_ in enumerate((x, xl, xr, xo))]
    z_all = rc(kvb.at[xc, 1:], kvb.at[xc, 1:], kzs, kzr, (e, t))

    def kv_first():
        z_all.wait_recv()
        own_kv.wait()
        kx[0].start()
        kx[1].start()
        kc[0].start()

    def kv_second():
        kx[0].wait_recv()
        kx[2].start()
        kc[1].start()
        kx[1].wait_recv()
        kx[3].start()
        kc[2].start()

    def kv_third():
        kx[2].wait_recv()
        kx[3].wait_recv()
        kc[3].start()

    def kv_ready():
        for copy in kc:
            copy.wait_recv()

    rows = arr.shape[2] * CAP

    def flat(ref):
        v = ref[...].astype(jnp.float32)
        return v.reshape(v.shape[0] * v.shape[1], v.shape[2])

    def experts(g):
        ags_all[g][2].wait_recv()
        ags_all[g][3].wait_recv()
        gate = jnp.zeros((rows, wg.shape[1]), jnp.float32)
        up = jnp.zeros((rows, wg.shape[1]), jnp.float32)
        for s in range(4):
            xs = flat(arr.at[s, g]).astype(jnp.bfloat16)
            gate += jnp.dot(xs, wg[s * wide : (s + 1) * wide, :], preferred_element_type=jnp.float32)
            up += jnp.dot(xs, wu[s * wide : (s + 1) * wide, :], preferred_element_type=jnp.float32)
        hidden = (gate / (1.0 + jnp.exp(-gate)) * up).astype(jnp.bfloat16)
        for s in range(4):
            value = jnp.dot(hidden, wd[:, s * wide : (s + 1) * wide], preferred_element_type=jnp.float32)
            part[s, g] = value.reshape(arr.shape[2], CAP, wide).astype(jnp.bfloat16)

    def rs(g):
        return [
            rc(part.at[opp, g, :half], rs1l.at[g], rss.at[0, g], rsr.at[0, g], at_right),
            rc(part.at[opp, g, half:], rs1r.at[g], rss.at[1, g], rsr.at[1, g], at_left),
            rc(part.at[right, g], rs2l.at[g], rss.at[2, g], rsr.at[2, g], at_right),
            rc(part.at[left, g], rs2r.at[g], rss.at[3, g], rsr.at[3, g], at_left),
        ]

    rs_all = [rs(g) for g in range(groups)]

    def add_to(dst, value):
        dst[...] = (dst[...].astype(jnp.float32) + value[...].astype(jnp.float32)).astype(jnp.bfloat16)

    def reduce_first(g):
        rs_all[g][0].start()
        rs_all[g][1].start()

    def reduce_second(g):
        rs_all[g][0].wait_recv()
        add_to(part.at[right, g, :half], rs1l.at[g])
        rs_all[g][2].start()
        rs_all[g][1].wait_recv()
        add_to(part.at[left, g, half:], rs1r.at[g])
        rs_all[g][3].start()

    own_back = pltpu.make_async_copy(res.at[0, 0], ret.at[e], lsem.at[2])

    def give_back(g):
        rs_all[g][2].wait_recv()
        rs_all[g][3].wait_recv()
        total = part[t, g].astype(jnp.float32) + rs2l[g].astype(jnp.float32) + rs2r[g].astype(jnp.float32)
        res[g] = total.astype(jnp.bfloat16)
        if g == 0:
            own_back.start()

        def back(i, carry):
            to = peer(g, i, -1)
            rc(res.at[g, i], ret.at[e], rts.at[g], rtr, (to, t)).start()
            return carry

        lax.fori_loop(1 if g == 0 else 0, 2 * NX * NC, back, 0)

    def block_of(b):
        return b % (NX * NC), b // (NX * NC)

    def load_block(b):
        i, j = block_of(b)
        return kvb[i, j, :ROWS], kvb[i, j, ROWS:][:1].astype(jnp.float32) * LOG2E

    def attend_first():
        kv, bias_row = load_block(e)
        out, total = block_update(lhs_ref[...], off, kv, bias_row, tri_ref[...], None, True)
        acc_ref[...] = out
        near_ref[...] = total

    def attend(piece, pieces):
        def step(i, carry):
            kv, bias_row = load_block(e - i)
            near = near_ref[...]
            out, total = block_update(lhs_ref[...], off, kv, bias_row, tri_ref[...], near, False)
            acc_ref[...] += out
            near_ref[...] = near + total
            return carry

        lax.fori_loop(1 + e * piece // pieces, 1 + e * (piece + 1) // pieces, step, 0)

    aw = apart.shape[1]
    ah = aw // 2
    ar = [
        rc(apart.at[opp, :ah], ars1l, ats.at[0], atr.at[0], at_right),
        rc(apart.at[opp, ah:], ars1r, ats.at[1], atr.at[1], at_left),
        rc(apart.at[right], ars2l, ats.at[2], atr.at[2], at_right),
        rc(apart.at[left], ars2r, ats.at[3], atr.at[3], at_left),
    ]

    def project():
        lane = lax.broadcasted_iota(jnp.int32, (ROWS, ROWS), 1)
        pairs = []
        for h in range(0, heads, 2):
            even = pltpu.roll(acc_ref[h * ROWS : (h + 1) * ROWS, :], HD, 1)
            odd = acc_ref[(h + 1) * ROWS : (h + 2) * ROWS, :]
            pairs.append(jnp.where(lane < HD, even, odd))
        attended = jnp.concatenate(pairs, axis=1).astype(jnp.bfloat16)
        step = 512
        for s in range(0, wo.shape[1], step):
            value = jnp.dot(attended, wo[:, s : s + step], preferred_element_type=jnp.float32)
            apart[:, :, s : s + step] = value.reshape(4, aw, step).astype(jnp.bfloat16)
        ar[0].start()
        ar[1].start()

    def project_second():
        ar[0].wait_recv()
        add_to(apart.at[right, :ah], ars1l)
        ar[2].start()
        ar[1].wait_recv()
        add_to(apart.at[left, ah:], ars1r)
        ar[3].start()

    def project_last():
        ar[2].wait_recv()
        ar[3].wait_recv()
        total = apart[t].astype(jnp.float32) + ars2l[...].astype(jnp.float32) + ars2r[...].astype(jnp.float32)
        att_out[...] = total.astype(jnp.bfloat16)

    spread_rows(0)
    kv_first()
    spread_rows(1)
    for load in loads:
        load.wait()
    forward_rows(0)
    spread_rows(2)
    forward_rows(1)
    spread_rows(3)
    kv_second()
    experts(0)
    reduce_first(0)
    forward_rows(2)
    kv_third()
    forward_rows(3)
    experts(1)
    reduce_first(1)
    reduce_second(0)
    kv_ready()
    attend_first()
    attend(0, 4)
    experts(2)
    reduce_first(2)
    reduce_second(1)
    give_back(0)
    attend(1, 4)
    experts(3)
    reduce_first(3)
    reduce_second(2)
    give_back(1)
    attend(2, 4)
    reduce_second(3)
    give_back(2)
    attend(3, 4)
    project()
    give_back(3)
    project_second()

    all_back = rc(ret.at[1:], ret.at[1:], rts.at[0], rtr, (e, t))
    all_back.wait_recv()
    own_back.wait()
    back_rows = flat(ret).astype(jnp.bfloat16)
    total = None
    for k in range(2):
        got = jnp.dot(pick[k], back_rows, preferred_element_type=jnp.float32) * route_ref[:, k : k + 1]
        total = got if total is None else total + got
    exp_out[...] = total.astype(jnp.bfloat16)
    project_last()

    for g in range(groups):
        arrived(g).wait_send()
        ref = res.at[g, 1:] if g == 0 else res.at[g]
        rc(ref, ref, rts.at[g], rtr, (e, t)).wait_send()
        for copy in ags_all[g] + rs_all[g]:
            copy.wait_send()
    for copy in kx + kc + ar + [z_all]:
        copy.wait_send()


def body(
    query_rows, key_rows, retrieved_vector_table, key_bias, score_offset, out_weight, second_batch_activations,
    norm_gain, expert_index, route_weight, gate_weight, up_weight, down_weight,
):
    ne = lax.axis_size("ep")
    tokens, width = second_batch_activations.shape
    wide = width // 4
    groups = len(DISTANCES)
    each = 2 * NX * NC
    heads = query_rows.shape[1] // HD
    bias_row = jnp.pad(key_bias.reshape(1, ROWS), ((0, 15), (0, 0)))
    pack = jnp.concatenate([jnp.concatenate([key_rows, retrieved_vector_table], axis=1), bias_row], axis=0)
    bf, f32 = jnp.bfloat16, jnp.float32
    vmem, dma = pltpu.VMEM, pltpu.SemaphoreType.DMA
    vspec, aspec = pl.BlockSpec(memory_space=pltpu.VMEM), pl.BlockSpec(memory_space=pl.ANY)
    aw = tokens // 4
    return pl.pallas_call(
        whole_kernel,
        out_shape=(
            jax.ShapeDtypeStruct((aw, width), bf),
            jax.ShapeDtypeStruct((tokens, wide), bf),
        ),
        in_specs=[pl.BlockSpec(memory_space=pltpu.SMEM)] + [vspec] * 7 + [aspec] * 4,
        out_specs=(vspec, vspec),
        scratch_shapes=[
            vmem((NX * NC, ne // (NX * NC), ROWS + 16, ROWS), bf),
            vmem((heads * ROWS, 2 * ROWS), bf),
            vmem((ROWS, 2 * ROWS), bf),
            vmem((heads * ROWS, ROWS), f32),
            vmem((heads * ROWS, ROWS), f32),
            vmem(gate_weight.shape[1:], bf),
            vmem(up_weight.shape[1:], bf),
            vmem(down_weight.shape[1:], bf),
            vmem(out_weight.shape, bf),
            vmem((ne, CAP, wide), bf),
            vmem((2, tokens, ne * CAP), bf),
            vmem((4, groups, each, CAP, wide), bf),
            vmem((4, groups, each, CAP, wide), bf),
            vmem((groups, each // 2, CAP, wide), bf),
            vmem((groups, each // 2, CAP, wide), bf),
            vmem((groups, each, CAP, wide), bf),
            vmem((groups, each, CAP, wide), bf),
            vmem((groups, each, CAP, wide), bf),
            vmem((ne, CAP, wide), bf),
            vmem((4, aw, width), bf),
            vmem((aw // 2, width), bf),
            vmem((aw // 2, width), bf),
            vmem((aw, width), bf),
            vmem((aw, width), bf),
            dma((4,)), dma((3,)), dma, dma, dma((4,)), dma((4,)), dma((4,)), dma((4,)),
            dma((groups,)), dma((groups,)), dma((4, groups)), dma((4, groups)), dma((4, groups)), dma((4, groups)),
            dma((groups,)), dma, dma((4,)), dma((4,)),
        ],
        compiler_params=pltpu.CompilerParams(
            collective_id=0, has_side_effects=True, vmem_limit_bytes=56 * 1024 * 1024
        ),
    )(
        score_offset, pack, query_rows, second_batch_activations, norm_gain.reshape(1, width), expert_index,
        expert_index.T, route_weight, gate_weight[0], up_weight[0], down_weight[0], out_weight,
    )


def solution(mesh):
    return jax.shard_map(
        body,
        mesh=mesh,
        in_specs=(
            P("ep", "tp"),
            P("ep", "tp"),
            P("ep", "tp"),
            P("ep", "tp"),
            P("tp"),
            P("tp", None),
            P("ep", None),
            P(),
            P("ep", None),
            P("ep", None),
            P("ep", None, "tp"),
            P("ep", None, "tp"),
            P("ep", "tp", None),
        ),
        out_specs=(P(("ep", "tp"), None), P("ep", "tp")),
        check_vma=False,
    )
```

```python
import jax
import jax.numpy as jnp
from jax import lax
from jax.experimental import pallas as pl
from jax.experimental.pallas import tpu as pltpu
from jax.sharding import PartitionSpec as P

HD = 64
LOG2E = 1.4426950408889634
ROWS = 128


def dot_rows(a, b):
    return lax.dot_general(a, b, (((1,), (1,)), ((), ())), preferred_element_type=jnp.float32)


def block_update(lhs, off, pairs, tri, near, masks):
    dots = [
        jnp.dot(lhs, jnp.concatenate([kv, kv], axis=0), preferred_element_type=jnp.float32) for kv, _ in pairs
    ]
    logs, sums, heads_of = [], [], []
    for n, (d, (_, bias)) in enumerate(zip(dots, pairs)):
        s = jnp.concatenate(
            [d[h * ROWS : (h + 1) * ROWS] + (bias - off[h]) for h in range(len(off))], axis=0
        )
        soft = jnp.maximum(s, jnp.log2(1.0 + jnp.exp2(jnp.minimum(s, 126.0))))
        logw = s - soft
        if masks is not None:
            row = lax.broadcasted_iota(jnp.int32, s.shape, 0) % ROWS + masks[n]
            later = row > lax.broadcasted_iota(jnp.int32, s.shape, 1)
            soft = jnp.where(later, soft, 0.0)
            logw = jnp.where(later, logw, -jnp.inf)
        logs.append(logw)
        heads_of.append(soft[:, :1])
        sums.append(jnp.dot(soft.astype(jnp.bfloat16), tri, preferred_element_type=jnp.float32))
    out = None
    for logw, total, first, (kv, _) in zip(logs, sums, heads_of, pairs):
        value = dot_rows(jnp.exp2(logw - total).astype(jnp.bfloat16), kv)
        if near is not None:
            value = value * jnp.exp2(-near)
        out = value if out is None else out + value
        step = jnp.broadcast_to(total[:, :1] + first, (total.shape[0], ROWS))
        near = step if near is None else near + step
    return out, near


def query_lhs(q):
    q2 = q.astype(jnp.float32) * (0.125 * LOG2E)
    hi = q2.astype(jnp.bfloat16)
    lo = (q2 - hi.astype(jnp.float32)).astype(jnp.bfloat16)
    zero = jnp.zeros((ROWS, HD), jnp.bfloat16)
    parts = []
    for h in range(q.shape[1] // HD):
        cut = slice(h * HD, (h + 1) * HD)
        parts.append(jnp.concatenate([hi[:, cut], zero, lo[:, cut], zero], axis=1))
    return jnp.concatenate(parts, axis=0)


def triangle():
    r = lax.broadcasted_iota(jnp.int32, (2 * ROWS, 2 * ROWS), 0)
    c = lax.broadcasted_iota(jnp.int32, (2 * ROWS, 2 * ROWS), 1)
    return jnp.where(r > c, 1.0, 0.0).astype(jnp.bfloat16)


NX, NC, CAP = 4, 2, 8
DISTANCES = ((0,), (2, 6), (3, 5, 4), (1, 7))
MESH = pl.DeviceIdType.MESH


def whole_kernel(
    off_ref, kt_ref, vt_ref, bias_ref, q_ref, act_ref, gain_ref, idxt_ref, routet_ref, wg_hbm, wu_hbm, wd_hbm, wo_hbm,
    att_out, exp_out,
    kvb, lhs_ref, tri_ref, acc_ref, near_ref, qfar, far, landed, attended_ref,
    wg, wu, wd, wo,
    outgoing, pick, scale, direct, arr, hid, res, ret,
    apart, aland,
    wsem, lsem, kzs, kzr, kxs, kxr, kcs, kcr, ds, dr, ags, agr, hgs, hgr, wds, wdr, rts, rtr, ats, atr, qss, qsr,
):
    e, t = lax.axis_index("ep"), lax.axis_index("tp")
    nz = lax.axis_size("ep") // (NX * NC)
    ne = nz * NX * NC
    tokens = act_ref.shape[0]
    heads = q_ref.shape[1] // HD
    groups = len(DISTANCES)
    count = [len(d) * NX * NC for d in DISTANCES]
    wide = arr.shape[-1]
    z, x, c = e // (NX * NC), e // NC % NX, e % NC
    xc = x * NC + c
    left, right, opp = (t + 3) % 4, (t + 1) % 4, (t + 2) % 4

    def ep_of(z_, x_, c_):
        return (z_ * NX + x_) * NC + c_

    def rc(src, dst, ssem, rsem, dev):
        return pltpu.make_async_remote_copy(
            src_ref=src, dst_ref=dst, send_sem=ssem, recv_sem=rsem, device_id=dev, device_id_type=MESH
        )

    barrier = pltpu.get_barrier_semaphore()

    def greet(i, carry):
        pl.semaphore_signal(barrier, inc=1, device_id=((e + i) % ne, t), device_id_type=MESH)
        return carry

    lax.fori_loop(1, ne, greet, 0)
    for near_t in (left, right, opp):
        pl.semaphore_signal(barrier, inc=1, device_id=(e, near_t), device_id_type=MESH)

    ff = wd_hbm.shape[0]

    def columns(to):
        return wd_hbm.at[:, pl.ds(pl.multiple_of(to * wide, wide), wide)]

    def part_rows(of):
        return wd.at[pl.ds(pl.multiple_of(of * ff, ff), ff)]

    loads = [
        pltpu.make_async_copy(src, dst, wsem.at[i])
        for i, (src, dst) in enumerate(((wg_hbm, wg), (wu_hbm, wu), (columns(t), part_rows(t)), (wo_hbm, wo)))
    ]
    for load in loads:
        load.start()
    kvb[xc, z] = jnp.concatenate(
        [kt_ref[...], vt_ref[...], jnp.broadcast_to(bias_ref[...].astype(jnp.float32), (16, ROWS)).astype(jnp.bfloat16)],
        axis=0,
    )

    pl.semaphore_wait(barrier, ne + 2)

    zr, zl = (ep_of((z + 1) % nz, x, c), t), (ep_of((z + nz - 1) % nz, x, c), t)

    def round_z(way, step):
        if way == 0:
            i, dev = (z + nz - step) % nz, zr
        else:
            i, dev = (z + step) % nz, zl
        return rc(kvb.at[xc, i], kvb.at[xc, i], kzs.at[way, step], kzr.at[way, step], dev)

    steps_z = (nz // 2, nz - 1 - nz // 2)
    kz = [[round_z(way, step) for step in range(steps_z[way])] for way in range(2)]

    def kv_round(step):
        for way in range(2):
            if 0 < step <= steps_z[way]:
                kz[way][step - 1].wait_recv()
            if step < steps_z[way]:
                kz[way][step].start()

    kv_round(0)

    at_right, at_left = (e, right), (e, left)
    wsend = [
        rc(columns(to), part_rows(t), wds.at[i], wdr.at[i], (e, to)) for i, to in enumerate((right, left, opp))
    ]

    def weights_ready():
        for copy in wsend:
            copy.wait_recv()
        for load in loads[2:]:
            load.wait()

    def loads_ready():
        for load in loads[:2]:
            load.wait()

    for copy in wsend:
        copy.start()

    values = act_ref[...].astype(jnp.float32)
    inv = lax.rsqrt(jnp.mean(values * values, axis=1, keepdims=True) + 1e-06)
    mine = pl.ds(pl.multiple_of(t * wide, wide), wide)
    i0 = lax.broadcasted_iota(jnp.int32, (tokens, tokens), 0)
    i1 = lax.broadcasted_iota(jnp.int32, (tokens, tokens), 1)
    below = jnp.where(i0 > i1, 1.0, 0.0).astype(jnp.bfloat16)
    above = jnp.where(i0 < i1, 1.0, 0.0).astype(jnp.bfloat16)
    idxt = [idxt_ref[k : k + 1, :] for k in range(2)]
    index = jnp.concatenate([idxt_ref[...].astype(jnp.float32), routet_ref[...], jnp.zeros((tokens - 4, tokens), jnp.float32)], axis=0).T
    scale[...] = index
    eq = [jnp.where(i1.astype(jnp.float32) == index[:, k : k + 1], 1.0, 0.0) for k in range(2)]
    prefix = jnp.dot(below, (eq[0] + eq[1]).astype(jnp.bfloat16), preferred_element_type=jnp.float32)
    eqt = [jnp.where(i0 == idxt[k], 1.0, 0.0) for k in range(2)]
    prefixt = jnp.dot((eqt[0] + eqt[1]).astype(jnp.bfloat16), above, preferred_element_type=jnp.float32)
    slots = ne * CAP
    col = lax.broadcasted_iota(jnp.int32, (tokens, slots), 1).astype(jnp.float32)
    row = lax.broadcasted_iota(jnp.int32, (slots, tokens), 0).astype(jnp.float32)
    spread = None
    for k in range(2):
        place = jnp.sum(eq[k] * prefix, axis=1, keepdims=True) + index[:, k : k + 1] * CAP
        pick[k] = jnp.where(col == place, 1.0, 0.0).astype(jnp.bfloat16)
        placet = jnp.sum(eqt[k] * prefixt, axis=0, keepdims=True) + idxt[k].astype(jnp.float32) * CAP
        one = jnp.where(row == placet, 1.0, 0.0)
        spread = one if spread is None else spread + one
    spread = spread.astype(jnp.bfloat16)
    for s in range(0, act_ref.shape[1], wide):
        cols = slice(s, s + wide)
        normed = (act_ref[:, cols].astype(jnp.float32) * inv * gain_ref[:, cols]).astype(jnp.bfloat16)
        sent = jnp.dot(spread, normed, preferred_element_type=jnp.float32)
        outgoing[:, :, cols] = sent.reshape(ne, CAP, wide).astype(jnp.bfloat16)
    lhs_ref[0] = query_lhs(q_ref[...])
    acc_ref[1] = jnp.zeros(acc_ref.shape[1:], jnp.float32)
    near_ref[1] = jnp.zeros(near_ref.shape[1:], jnp.float32)
    tri_ref[...] = triangle()
    off = [off_ref[h] * LOG2E for h in range(heads)]

    def peer(g, i, sign):
        per = NX * NC
        dz = DISTANCES[g][-1] % nz
        for n in range(len(DISTANCES[g]) - 1, 0, -1):
            dz = jnp.where(i < n * per, DISTANCES[g][n - 1] % nz, dz)
        dx, dc = i // NC % NX, i % NC
        if sign < 0:
            dz, dx = nz - dz, NX - dx
        return ep_of((z + dz) % nz, (x + dx) % NX, (c + dc) % NC)

    own_rows = pltpu.make_async_copy(outgoing.at[e], direct.at[0], lsem.at[1])
    own_rows.start()
    def dispatch(g, first=0, last=3):
        def scatter(i, carry):
            to = peer(g, i, 1)
            if g == 0:
                src, dst = outgoing.at[to], direct.at[i]
            else:
                src, dst = outgoing.at[to, :, mine], arr.at[t, g - 1, i]
            rc(src, dst, ds.at[g], dr.at[g], (to, t)).start()
            return carry

        per = NX * NC
        lax.fori_loop(1 if g == 0 else first * per, min(last * per, count[g]), scatter, 0)

    def arrived(g):
        ref = direct.at[1:] if g == 0 else arr.at[t, g - 1, : count[g]]
        return rc(ref, ref, ds.at[g], dr.at[g], (e, t))

    def ag(g):
        n, half = count[g], count[g] // 2
        a, left_rows, right_rows = arr.at[t, g - 1, :n], arr.at[left, g - 1, :half], arr.at[right, g - 1, half:n]
        return [
            rc(a, a, ags.at[0, g], agr.at[0, g], at_right),
            rc(a, a, ags.at[1, g], agr.at[1, g], at_left),
            rc(left_rows, left_rows, ags.at[2, g], agr.at[2, g], at_right),
            rc(right_rows, right_rows, ags.at[3, g], agr.at[3, g], at_left),
        ]

    ags_all = [[]] + [ag(g) for g in range(1, groups)]

    def spread_rows(g):
        arrived(g).wait_recv()
        ags_all[g][0].start()
        ags_all[g][1].start()

    def forward_rows(g):
        ags_all[g][0].wait_recv()
        ags_all[g][2].start()
        ags_all[g][1].wait_recv()
        ags_all[g][3].start()

    xl, xr, xo = (x + 3) % NX, (x + 1) % NX, (x + 2) % NX
    dev_xr, dev_xl, dev_c = (ep_of(z, xr, c), t), (ep_of(z, xl, c), t), (ep_of(z, x, (c + 1) % NC), t)
    zh = nz // 2

    def grp(x_):
        return kvb.at[x_ * NC + c]

    kx = [
        rc(grp(x), grp(x), kxs.at[0], kxr.at[0], dev_xr),
        rc(grp(x), grp(x), kxs.at[1], kxr.at[1], dev_xl),
        rc(kvb.at[xl * NC + c, :zh], kvb.at[xl * NC + c, :zh], kxs.at[2], kxr.at[2], dev_xr),
        rc(kvb.at[xr * NC + c, zh:], kvb.at[xr * NC + c, zh:], kxs.at[3], kxr.at[3], dev_xl),
    ]
    kc = [rc(grp(x_), grp(x_), kcs.at[i], kcr.at[i], dev_c) for i, x_ in enumerate((x, xl, xr, xo))]

    def kv_first():
        kv_round(4)
        kx[0].start()
        kx[1].start()
        kc[0].start()

    def kv_second():
        kx[0].wait_recv()
        kx[2].start()
        kc[1].start()
        kx[1].wait_recv()
        kx[3].start()
        kc[2].start()

    def kv_third():
        kx[2].wait_recv()
        kx[3].wait_recv()
        kc[3].start()

    def kv_ready():
        for copy in kc:
            copy.wait_recv()


    def flat(ref):
        v = ref[...].astype(jnp.float32)
        return v.reshape(v.shape[0] * v.shape[1], v.shape[2])

    def experts(g):
        if g == 0:
            arrived(0).wait_recv()
            own_rows.wait()
            xs = flat(direct).astype(jnp.bfloat16)
        else:
            ags_all[g][2].wait_recv()
            ags_all[g][3].wait_recv()
            xs = jnp.concatenate([flat(arr.at[s, g - 1, : count[g]]).astype(jnp.bfloat16) for s in range(4)], axis=1)
        gate = jnp.dot(xs, wg[...], preferred_element_type=jnp.float32)
        up = jnp.dot(xs, wu[...], preferred_element_type=jnp.float32)
        hidden = (gate / (1.0 + jnp.exp(-gate)) * up).astype(jnp.bfloat16)
        hid[t, g, : count[g] * CAP] = hidden
        hgs_all[g][0].start()
        hgs_all[g][1].start()

    def hg(g):
        rows, half = count[g] * CAP, count[g] * CAP // 2
        a, left_rows, right_rows = hid.at[t, g, :rows], hid.at[left, g, :half], hid.at[right, g, half:rows]
        return [
            rc(a, a, hgs.at[0, g], hgr.at[0, g], at_right),
            rc(a, a, hgs.at[1, g], hgr.at[1, g], at_left),
            rc(left_rows, left_rows, hgs.at[2, g], hgr.at[2, g], at_right),
            rc(right_rows, right_rows, hgs.at[3, g], hgr.at[3, g], at_left),
        ]

    hgs_all = [hg(g) for g in range(groups)]

    def forward_hidden(g):
        hgs_all[g][0].wait_recv()
        hgs_all[g][2].start()
        hgs_all[g][1].wait_recv()
        hgs_all[g][3].start()

    own_back = pltpu.make_async_copy(res.at[0, 0], ret.at[e], lsem.at[2])

    def give_back(g):
        hgs_all[g][2].wait_recv()
        hgs_all[g][3].wait_recv()
        hidden = jnp.concatenate([hid[s, g, : count[g] * CAP] for s in range(4)], axis=1)
        value = jnp.dot(hidden, wd[...], preferred_element_type=jnp.float32)
        res[g, : count[g]] = value.reshape(count[g], CAP, wide).astype(jnp.bfloat16)
        if g == 0:
            own_back.start()

        def back(i, carry):
            to = peer(g, i, -1)
            rc(res.at[g, i], ret.at[e], rts.at[g], rtr, (to, t)).start()
            return carry

        lax.fori_loop(1 if g == 0 else 0, count[g], back, 0)

    def load_pair(b):
        i, j = b % (NX * NC), b // (NX * NC)
        kv = jnp.concatenate([kvb[i, j, :ROWS], kvb[i + 1, j, :ROWS]], axis=1)
        bias = jnp.concatenate([kvb[i, j, ROWS:][:1], kvb[i + 1, j, ROWS:][:1]], axis=1)
        return kv, bias.astype(jnp.float32) * LOG2E

    heavy, light = z >= nz // 2, z < nz // 2
    shared = jnp.where(heavy, 2 * z + 1 - nz, nz - 1 - 2 * z) * (NX * NC // 8)
    partner = (ep_of(nz - 1 - z, x, c), t)
    ask = rc(q_ref, qfar, qss.at[0], qsr.at[0], partner)
    answer = rc(far, landed, qss.at[1], qsr.at[1], partner)

    def attend_quad(slot, quad, first):
        pairs = [load_pair(quad * 4 + 2), load_pair(quad * 4)]
        own = e % 4 * ROWS
        lhs, tri = lhs_ref[slot], tri_ref[...]
        near = None if first else near_ref[slot]
        result = block_update(lhs, off, pairs, tri, near, (own - 2 * ROWS, own) if first else None)
        acc_ref[slot] = result[0] if first else acc_ref[slot] + result[0]
        near_ref[slot] = result[1]

    def packed(ref):
        lane = lax.broadcasted_iota(jnp.int32, (ROWS, ROWS), 1)
        pairs = []
        for h in range(0, heads, 2):
            even = pltpu.roll(ref[h * ROWS : (h + 1) * ROWS, :], HD, 1)
            odd = ref[(h + 1) * ROWS : (h + 2) * ROWS, :]
            pairs.append(jnp.where(lane < HD, even, odd))
        return jnp.concatenate(pairs, axis=1)

    def ask_partner():
        @pl.when(heavy)
        def _():
            ask.start()

    def attend_far_start():
        @pl.when(light)
        def _():
            ask.wait_recv()
            lhs_ref[1] = query_lhs(qfar[...])

    def attend_far(piece, pieces):
        much = jnp.where(light, shared, 0)

        def step(i, carry):
            attend_quad(1, much - 1 - i, False)
            return carry

        lax.fori_loop(much * piece // pieces, much * (piece + 1) // pieces, step, 0)

    def attend_far_send():
        @pl.when(light)
        def _():
            far[...] = packed(acc_ref.at[1]).astype(jnp.bfloat16)
            answer.start()

    quads = e // 4

    def attend_first():
        attend_quad(0, quads, True)

    def attend(piece, pieces):
        much = quads - jnp.where(heavy, shared, 0)

        def step(i, carry):
            attend_quad(0, quads - i, False)
            return carry

        lax.fori_loop(1 + much * piece // pieces, 1 + much * (piece + 1) // pieces, step, 0)

    aw = apart.shape[1]
    ar = [
        rc(apart.at[to], aland.at[i], ats.at[i], atr.at[i], (e, to)) for i, to in enumerate((right, left, opp))
    ]

    def project():
        attended_ref[...] = packed(acc_ref.at[0])

        @pl.when(heavy)
        def _():
            answer.wait_recv()
            attended_ref[...] += jnp.exp2(-packed(near_ref.at[0])) * landed[...].astype(jnp.float32)

        attended = attended_ref[...].astype(jnp.bfloat16)
        step = 512
        for s in range(0, wo.shape[1], step):
            value = jnp.dot(attended, wo[:, s : s + step], preferred_element_type=jnp.float32)
            apart[:, :, s : s + step] = value.reshape(4, aw, step).astype(jnp.bfloat16)
        for copy in ar:
            copy.start()

    def project_last():
        total = apart[t].astype(jnp.float32)
        for i, copy in enumerate(ar):
            copy.wait_recv()
            total = total + aland[i].astype(jnp.float32)
        att_out[...] = total.astype(jnp.bfloat16)

    def finish():
        all_back = rc(ret.at[1:], ret.at[1:], rts.at[0], rtr, (e, t))
        all_back.wait_recv()
        own_back.wait()
        back_rows = flat(ret).astype(jnp.bfloat16)
        total = None
        for k in range(2):
            got = jnp.dot(pick[k], back_rows, preferred_element_type=jnp.float32) * scale[:, 2 + k : 3 + k]
            total = got if total is None else total + got
        exp_out[...] = total.astype(jnp.bfloat16)
        project_last()

    dispatch(1)
    kv_round(1)
    dispatch(2, 0, 2)
    kv_round(2)
    dispatch(2, 2, 3)
    ask_partner()
    spread_rows(1)
    kv_round(3)
    dispatch(3)
    forward_rows(1)
    kv_first()
    dispatch(0)
    spread_rows(2)
    loads_ready()
    spread_rows(3)
    experts(1)
    forward_rows(2)
    kv_second()
    experts(0)
    weights_ready()
    forward_hidden(1)
    forward_rows(3)
    kv_third()
    experts(2)
    give_back(1)
    forward_hidden(0)
    kv_ready()
    attend_far_start()
    attend_far(0, 2)
    experts(3)
    forward_hidden(2)
    give_back(0)
    attend_far(1, 2)
    attend_far_send()
    attend_first()
    attend(0, 4)
    forward_hidden(3)
    give_back(2)
    attend(1, 4)
    attend(2, 4)
    give_back(3)
    attend(3, 4)
    project()
    finish()

    for g in range(groups):
        arrived(g).wait_send()
        ref = res.at[g, 1 if g == 0 else 0 : count[g]]
        rc(ref, ref, rts.at[g], rtr, (e, t)).wait_send()
        for copy in ags_all[g] + hgs_all[g]:
            copy.wait_send()
    @pl.when(heavy)
    def _():
        ask.wait_send()

    @pl.when(light)
    def _():
        answer.wait_send()

    for copy in kz[0] + kz[1] + kx + kc + ar + wsend:
        copy.wait_send()


def body(
    query_rows, key_rows, retrieved_vector_table, key_bias, score_offset, out_weight, second_batch_activations,
    norm_gain, expert_index, route_weight, gate_weight, up_weight, down_weight,
):
    ne = lax.axis_size("ep")
    tokens, width = second_batch_activations.shape
    wide = width // 4
    groups = len(DISTANCES)
    most = max(len(d) for d in DISTANCES) * NX * NC
    many = max(len(d) for d in DISTANCES[1:]) * NX * NC
    heads = query_rows.shape[1] // HD
    bf, f32 = jnp.bfloat16, jnp.float32
    vmem, dma = pltpu.VMEM, pltpu.SemaphoreType.DMA
    vspec, aspec = pl.BlockSpec(memory_space=pltpu.VMEM), pl.BlockSpec(memory_space=pl.ANY)
    aw = tokens // 4
    return pl.pallas_call(
        whole_kernel,
        out_shape=(
            jax.ShapeDtypeStruct((aw, width), bf),
            jax.ShapeDtypeStruct((tokens, wide), bf),
        ),
        in_specs=[pl.BlockSpec(memory_space=pltpu.SMEM)] + [vspec] * 8 + [aspec] * 4,
        out_specs=(vspec, vspec),
        scratch_shapes=[
            vmem((NX * NC, ne // (NX * NC), ROWS + 16, ROWS), bf),
            vmem((2, heads * ROWS, 2 * ROWS), bf),
            vmem((2 * ROWS, 2 * ROWS), bf),
            vmem((2, heads * ROWS, ROWS), f32),
            vmem((2, heads * ROWS, ROWS), f32),
            vmem((ROWS, heads * HD), bf),
            vmem((ROWS, heads * HD), bf),
            vmem((ROWS, heads * HD), bf),
            vmem((ROWS, heads * HD), f32),
            vmem(gate_weight.shape[1:], bf),
            vmem(up_weight.shape[1:], bf),
            vmem((4 * down_weight.shape[1], wide), bf),
            vmem(out_weight.shape, bf),
            vmem((ne, CAP, width), bf),
            vmem((2, tokens, ne * CAP), bf),
            vmem((tokens, tokens), f32),
            vmem((len(DISTANCES[0]) * NX * NC, CAP, width), bf),
            vmem((4, groups - 1, many, CAP, wide), bf),
            vmem((4, groups, most * CAP, gate_weight.shape[2]), bf),
            vmem((groups, most, CAP, wide), bf),
            vmem((ne, CAP, wide), bf),
            vmem((4, aw, width), bf),
            vmem((3, aw, width), bf),
            dma((4,)), dma((3,)), dma((2, 4)), dma((2, 4)), dma((4,)), dma((4,)), dma((4,)), dma((4,)),
            dma((groups,)), dma((groups,)), dma((4, groups)), dma((4, groups)), dma((4, groups)), dma((4, groups)), dma((3,)), dma((3,)),
            dma((groups,)), dma, dma((3,)), dma((3,)), dma((2,)), dma((2,)),
        ],
        compiler_params=pltpu.CompilerParams(
            collective_id=0, has_side_effects=True, vmem_limit_bytes=56 * 1024 * 1024
        ),
    )(
        score_offset, key_rows.T, retrieved_vector_table.T, key_bias.T, query_rows, second_batch_activations,
        norm_gain.reshape(1, width), expert_index.T, route_weight.T, gate_weight[0], up_weight[0], down_weight[0],
        out_weight,
    )


def solution(mesh):
    return jax.shard_map(
        body,
        mesh=mesh,
        in_specs=(
            P("ep", "tp"),
            P("ep", "tp"),
            P("ep", "tp"),
            P("ep", "tp"),
            P("tp"),
            P("tp", None),
            P("ep", None),
            P(),
            P("ep", None),
            P("ep", None),
            P("ep", None, "tp"),
            P("ep", None, "tp"),
            P("ep", "tp", None),
        ),
        out_specs=(P(("ep", "tp"), None), P("ep", "tp")),
        check_vma=False,
    )
```

```python
import jax
import jax.numpy as jnp
from jax import lax
from jax.experimental import pallas as pl
from jax.experimental.pallas import tpu as pltpu
from jax.sharding import PartitionSpec as P

HD = 64
LOG2E = 1.4426950408889634
ROWS = 128


def dot_rows(a, b):
    return lax.dot_general(a, b, (((1,), (1,)), ((), ())), preferred_element_type=jnp.float32)


def block_update(lhs, off, pairs, tri, near, masks):
    dots = [
        jnp.dot(lhs, jnp.concatenate([kv, kv], axis=0), preferred_element_type=jnp.float32) for kv, _ in pairs
    ]
    logs, sums, heads_of = [], [], []
    for n, (d, (_, bias)) in enumerate(zip(dots, pairs)):
        s = jnp.concatenate(
            [d[h * ROWS : (h + 1) * ROWS] + (bias - off[h]) for h in range(len(off))], axis=0
        )
        soft = jnp.maximum(s, jnp.log2(1.0 + jnp.exp2(jnp.minimum(s, 126.0))))
        logw = s - soft
        if masks is not None:
            row = lax.broadcasted_iota(jnp.int32, s.shape, 0) % ROWS + masks[n]
            later = row > lax.broadcasted_iota(jnp.int32, s.shape, 1)
            soft = jnp.where(later, soft, 0.0)
            logw = jnp.where(later, logw, -jnp.inf)
        logs.append(logw)
        heads_of.append(soft[:, :1])
        sums.append(jnp.dot(soft.astype(jnp.bfloat16), tri, preferred_element_type=jnp.float32))
    out = None
    for logw, total, first, (kv, _) in zip(logs, sums, heads_of, pairs):
        value = dot_rows(jnp.exp2(logw - total).astype(jnp.bfloat16), kv)
        if near is not None:
            value = value * jnp.exp2(-near)
        out = value if out is None else out + value
        step = jnp.broadcast_to(total[:, :1] + first, (total.shape[0], ROWS))
        near = step if near is None else near + step
    return out, near


def query_lhs(q):
    q2 = q.astype(jnp.float32) * (0.125 * LOG2E)
    hi = q2.astype(jnp.bfloat16)
    lo = (q2 - hi.astype(jnp.float32)).astype(jnp.bfloat16)
    zero = jnp.zeros((ROWS, HD), jnp.bfloat16)
    parts = []
    for h in range(q.shape[1] // HD):
        cut = slice(h * HD, (h + 1) * HD)
        parts.append(jnp.concatenate([hi[:, cut], zero, lo[:, cut], zero], axis=1))
    return jnp.concatenate(parts, axis=0)


def triangle():
    r = lax.broadcasted_iota(jnp.int32, (2 * ROWS, 2 * ROWS), 0)
    c = lax.broadcasted_iota(jnp.int32, (2 * ROWS, 2 * ROWS), 1)
    return jnp.where(r > c, 1.0, 0.0).astype(jnp.bfloat16)


NX, NC, CAP = 4, 2, 8
DISTANCES = ((0,), (3, 5, 4), (2, 6), (1, 7))
MESH = pl.DeviceIdType.MESH


def whole_kernel(
    off_ref, kt_ref, vt_ref, bias_ref, q_ref, act_ref, gain_ref, idxt_ref, routet_ref, wg_hbm, wu_hbm, wd_hbm, wo_hbm,
    att_out, exp_out,
    kvb, lhs_ref, tri_ref, acc_ref, near_ref, qfar, far, landed, attended_ref,
    wg, wu, wd, wo,
    outgoing, pick, scale, direct, arr, hid, res, ret,
    apart, aland,
    wsem, lsem, kzs, kzr, kxs, kxr, kcs, kcr, ds, dr, ags, agr, hgs, hgr, wds, wdr, rts, rtr, ats, atr, qss, qsr,
):
    e, t = lax.axis_index("ep"), lax.axis_index("tp")
    nz = lax.axis_size("ep") // (NX * NC)
    ne = nz * NX * NC
    tokens = act_ref.shape[0]
    heads = q_ref.shape[1] // HD
    groups = len(DISTANCES)
    count = [len(d) * NX * NC for d in DISTANCES]
    wide = arr.shape[-1]
    z, x, c = e // (NX * NC), e // NC % NX, e % NC
    xc = x * NC + c
    left, right, opp = (t + 3) % 4, (t + 1) % 4, (t + 2) % 4

    def ep_of(z_, x_, c_):
        return (z_ * NX + x_) * NC + c_

    def rc(src, dst, ssem, rsem, dev):
        return pltpu.make_async_remote_copy(
            src_ref=src, dst_ref=dst, send_sem=ssem, recv_sem=rsem, device_id=dev, device_id_type=MESH
        )

    barrier = pltpu.get_barrier_semaphore()

    def greet(i, carry):
        pl.semaphore_signal(barrier, inc=1, device_id=((e + i) % ne, t), device_id_type=MESH)
        return carry

    lax.fori_loop(1, ne, greet, 0)
    for near_t in (left, right, opp):
        pl.semaphore_signal(barrier, inc=1, device_id=(e, near_t), device_id_type=MESH)

    ff = wd_hbm.shape[0]

    def columns(to):
        return wd_hbm.at[:, pl.ds(pl.multiple_of(to * wide, wide), wide)]

    def part_rows(of):
        return wd.at[pl.ds(pl.multiple_of(of * ff, ff), ff)]

    loads = [
        pltpu.make_async_copy(src, dst, wsem.at[i])
        for i, (src, dst) in enumerate(((wg_hbm, wg), (wu_hbm, wu), (columns(t), part_rows(t)), (wo_hbm, wo)))
    ]
    for load in loads:
        load.start()
    kvb[xc, z] = jnp.concatenate(
        [kt_ref[...], vt_ref[...], jnp.broadcast_to(bias_ref[...].astype(jnp.float32), (16, ROWS)).astype(jnp.bfloat16)],
        axis=0,
    )

    pl.semaphore_wait(barrier, ne + 2)

    zr, zl = (ep_of((z + 1) % nz, x, c), t), (ep_of((z + nz - 1) % nz, x, c), t)

    def round_z(way, step):
        if way == 0:
            i, dev = (z + nz - step) % nz, zr
        else:
            i, dev = (z + step) % nz, zl
        return rc(kvb.at[xc, i], kvb.at[xc, i], kzs.at[way, step], kzr.at[way, step], dev)

    steps_z = (nz // 2, nz - 1 - nz // 2)
    kz = [[round_z(way, step) for step in range(steps_z[way])] for way in range(2)]

    def kv_round(step):
        for way in range(2):
            if 0 < step <= steps_z[way]:
                kz[way][step - 1].wait_recv()
            if step < steps_z[way]:
                kz[way][step].start()

    kv_round(0)

    at_right, at_left = (e, right), (e, left)
    wsend = [
        rc(columns(to), part_rows(t), wds.at[i], wdr.at[i], (e, to)) for i, to in enumerate((right, left, opp))
    ]

    def weights_ready():
        for copy in wsend:
            copy.wait_recv()
        for load in loads[2:]:
            load.wait()

    def loads_ready():
        for load in loads[:2]:
            load.wait()

    for copy in wsend:
        copy.start()

    values = act_ref[...].astype(jnp.float32)
    inv = lax.rsqrt(jnp.mean(values * values, axis=1, keepdims=True) + 1e-06)
    mine = pl.ds(pl.multiple_of(t * wide, wide), wide)
    i0 = lax.broadcasted_iota(jnp.int32, (tokens, tokens), 0)
    i1 = lax.broadcasted_iota(jnp.int32, (tokens, tokens), 1)
    below = jnp.where(i0 > i1, 1.0, 0.0).astype(jnp.bfloat16)
    above = jnp.where(i0 < i1, 1.0, 0.0).astype(jnp.bfloat16)
    idxt = [idxt_ref[k : k + 1, :] for k in range(2)]
    index = jnp.concatenate([idxt_ref[...].astype(jnp.float32), routet_ref[...], jnp.zeros((tokens - 4, tokens), jnp.float32)], axis=0).T
    scale[...] = index
    eq = [jnp.where(i1.astype(jnp.float32) == index[:, k : k + 1], 1.0, 0.0) for k in range(2)]
    prefix = jnp.dot(below, (eq[0] + eq[1]).astype(jnp.bfloat16), preferred_element_type=jnp.float32)
    eqt = [jnp.where(i0 == idxt[k], 1.0, 0.0) for k in range(2)]
    prefixt = jnp.dot((eqt[0] + eqt[1]).astype(jnp.bfloat16), above, preferred_element_type=jnp.float32)
    slots = ne * CAP
    col = lax.broadcasted_iota(jnp.int32, (tokens, slots), 1).astype(jnp.float32)
    row = lax.broadcasted_iota(jnp.int32, (slots, tokens), 0).astype(jnp.float32)
    spread = None
    for k in range(2):
        place = jnp.sum(eq[k] * prefix, axis=1, keepdims=True) + index[:, k : k + 1] * CAP
        pick[k] = jnp.where(col == place, 1.0, 0.0).astype(jnp.bfloat16)
        placet = jnp.sum(eqt[k] * prefixt, axis=0, keepdims=True) + idxt[k].astype(jnp.float32) * CAP
        one = jnp.where(row == placet, 1.0, 0.0)
        spread = one if spread is None else spread + one
    spread = spread.astype(jnp.bfloat16)
    for s in range(0, act_ref.shape[1], wide):
        cols = slice(s, s + wide)
        normed = (act_ref[:, cols].astype(jnp.float32) * inv * gain_ref[:, cols]).astype(jnp.bfloat16)
        sent = jnp.dot(spread, normed, preferred_element_type=jnp.float32)
        outgoing[:, :, cols] = sent.reshape(ne, CAP, wide).astype(jnp.bfloat16)
    lhs_ref[0] = query_lhs(q_ref[...])
    acc_ref[1] = jnp.zeros(acc_ref.shape[1:], jnp.float32)
    near_ref[1] = jnp.zeros(near_ref.shape[1:], jnp.float32)
    tri_ref[...] = triangle()
    off = [off_ref[h] * LOG2E for h in range(heads)]

    def peer(g, i, sign):
        per = NX * NC
        dz = DISTANCES[g][-1] % nz
        for n in range(len(DISTANCES[g]) - 1, 0, -1):
            dz = jnp.where(i < n * per, DISTANCES[g][n - 1] % nz, dz)
        dx, dc = i // NC % NX, i % NC
        if sign < 0:
            dz, dx = nz - dz, NX - dx
        return ep_of((z + dz) % nz, (x + dx) % NX, (c + dc) % NC)

    own_rows = pltpu.make_async_copy(outgoing.at[e], direct.at[0], lsem.at[1])
    own_rows.start()
    def dispatch(g, first=0, last=3):
        def scatter(i, carry):
            to = peer(g, i, 1)
            if g == 0:
                src, dst = outgoing.at[to], direct.at[i]
            else:
                src, dst = outgoing.at[to, :, mine], arr.at[t, g - 1, i]
            rc(src, dst, ds.at[g], dr.at[g], (to, t)).start()
            return carry

        per = NX * NC
        lax.fori_loop(1 if g == 0 else first * per, min(last * per, count[g]), scatter, 0)

    def arrived(g):
        ref = direct.at[1:] if g == 0 else arr.at[t, g - 1, : count[g]]
        return rc(ref, ref, ds.at[g], dr.at[g], (e, t))

    def ag(g):
        n, half = count[g], count[g] // 2
        a, left_rows, right_rows = arr.at[t, g - 1, :n], arr.at[left, g - 1, :half], arr.at[right, g - 1, half:n]
        return [
            rc(a, a, ags.at[0, g], agr.at[0, g], at_right),
            rc(a, a, ags.at[1, g], agr.at[1, g], at_left),
            rc(left_rows, left_rows, ags.at[2, g], agr.at[2, g], at_right),
            rc(right_rows, right_rows, ags.at[3, g], agr.at[3, g], at_left),
        ]

    ags_all = [[]] + [ag(g) for g in range(1, groups)]

    def spread_rows(g):
        arrived(g).wait_recv()
        ags_all[g][0].start()
        ags_all[g][1].start()

    def forward_rows(g):
        ags_all[g][0].wait_recv()
        ags_all[g][2].start()
        ags_all[g][1].wait_recv()
        ags_all[g][3].start()

    xl, xr, xo = (x + 3) % NX, (x + 1) % NX, (x + 2) % NX
    dev_xr, dev_xl, dev_c = (ep_of(z, xr, c), t), (ep_of(z, xl, c), t), (ep_of(z, x, (c + 1) % NC), t)
    zh = nz // 2

    def grp(x_):
        return kvb.at[x_ * NC + c]

    kx = [
        rc(grp(x), grp(x), kxs.at[0], kxr.at[0], dev_xr),
        rc(grp(x), grp(x), kxs.at[1], kxr.at[1], dev_xl),
        rc(kvb.at[xl * NC + c, :zh], kvb.at[xl * NC + c, :zh], kxs.at[2], kxr.at[2], dev_xr),
        rc(kvb.at[xr * NC + c, zh:], kvb.at[xr * NC + c, zh:], kxs.at[3], kxr.at[3], dev_xl),
    ]
    kc = [rc(grp(x_), grp(x_), kcs.at[i], kcr.at[i], dev_c) for i, x_ in enumerate((x, xl, xr, xo))]

    def kv_first():
        kv_round(4)
        kx[0].start()
        kx[1].start()
        kc[0].start()

    def kv_second():
        kx[0].wait_recv()
        kx[2].start()
        kc[1].start()
        kx[1].wait_recv()
        kx[3].start()
        kc[2].start()

    def kv_third():
        kx[2].wait_recv()
        kx[3].wait_recv()
        kc[3].start()

    def kv_ready():
        for copy in kc:
            copy.wait_recv()


    def flat(ref):
        v = ref[...].astype(jnp.float32)
        return v.reshape(v.shape[0] * v.shape[1], v.shape[2])

    def experts(g):
        if g == 0:
            arrived(0).wait_recv()
            own_rows.wait()
            xs = flat(direct).astype(jnp.bfloat16)
        else:
            ags_all[g][2].wait_recv()
            ags_all[g][3].wait_recv()
            xs = jnp.concatenate([flat(arr.at[s, g - 1, : count[g]]).astype(jnp.bfloat16) for s in range(4)], axis=1)
        gate = jnp.dot(xs, wg[...], preferred_element_type=jnp.float32)
        up = jnp.dot(xs, wu[...], preferred_element_type=jnp.float32)
        hidden = (gate / (1.0 + jnp.exp(-gate)) * up).astype(jnp.bfloat16)
        hid[t, g, : count[g] * CAP] = hidden
        hgs_all[g][0].start()
        hgs_all[g][1].start()

    def hg(g):
        rows, half = count[g] * CAP, count[g] * CAP // 2
        a, left_rows, right_rows = hid.at[t, g, :rows], hid.at[left, g, :half], hid.at[right, g, half:rows]
        return [
            rc(a, a, hgs.at[0, g], hgr.at[0, g], at_right),
            rc(a, a, hgs.at[1, g], hgr.at[1, g], at_left),
            rc(left_rows, left_rows, hgs.at[2, g], hgr.at[2, g], at_right),
            rc(right_rows, right_rows, hgs.at[3, g], hgr.at[3, g], at_left),
        ]

    hgs_all = [hg(g) for g in range(groups)]

    def forward_hidden(g):
        hgs_all[g][0].wait_recv()
        hgs_all[g][2].start()
        hgs_all[g][1].wait_recv()
        hgs_all[g][3].start()

    own_back = pltpu.make_async_copy(res.at[0, 0], ret.at[e], lsem.at[2])

    def give_back(g):
        hgs_all[g][2].wait_recv()
        hgs_all[g][3].wait_recv()
        hidden = jnp.concatenate([hid[s, g, : count[g] * CAP] for s in range(4)], axis=1)
        value = jnp.dot(hidden, wd[...], preferred_element_type=jnp.float32)
        res[g, : count[g]] = value.reshape(count[g], CAP, wide).astype(jnp.bfloat16)
        if g == 0:
            own_back.start()

        def back(i, carry):
            to = peer(g, i, -1)
            rc(res.at[g, i], ret.at[e], rts.at[g], rtr, (to, t)).start()
            return carry

        lax.fori_loop(1 if g == 0 else 0, count[g], back, 0)

    def load_pair(b):
        i, j = b % (NX * NC), b // (NX * NC)
        kv = jnp.concatenate([kvb[i, j, :ROWS], kvb[i + 1, j, :ROWS]], axis=1)
        bias = jnp.concatenate([kvb[i, j, ROWS:][:1], kvb[i + 1, j, ROWS:][:1]], axis=1)
        return kv, bias.astype(jnp.float32) * LOG2E

    heavy, light = z >= nz // 2, z < nz // 2
    shared = jnp.where(heavy, 2 * z + 1 - nz, nz - 1 - 2 * z) * (NX * NC // 8)
    partner = (ep_of(nz - 1 - z, x, c), t)
    ask = rc(q_ref, qfar, qss.at[0], qsr.at[0], partner)
    answer = rc(far, landed, qss.at[1], qsr.at[1], partner)

    def attend_quad(slot, quad, first):
        pairs = [load_pair(quad * 4 + 2), load_pair(quad * 4)]
        own = e % 4 * ROWS
        lhs, tri = lhs_ref[slot], tri_ref[...]
        near = None if first else near_ref[slot]
        result = block_update(lhs, off, pairs, tri, near, (own - 2 * ROWS, own) if first else None)
        acc_ref[slot] = result[0] if first else acc_ref[slot] + result[0]
        near_ref[slot] = result[1]

    def packed(ref):
        lane = lax.broadcasted_iota(jnp.int32, (ROWS, ROWS), 1)
        pairs = []
        for h in range(0, heads, 2):
            even = pltpu.roll(ref[h * ROWS : (h + 1) * ROWS, :], HD, 1)
            odd = ref[(h + 1) * ROWS : (h + 2) * ROWS, :]
            pairs.append(jnp.where(lane < HD, even, odd))
        return jnp.concatenate(pairs, axis=1)

    def ask_partner():
        @pl.when(heavy)
        def _():
            ask.start()

    def attend_far_start():
        @pl.when(light)
        def _():
            ask.wait_recv()
            lhs_ref[1] = query_lhs(qfar[...])

    def attend_far(piece, pieces):
        much = jnp.where(light, shared, 0)

        def step(i, carry):
            attend_quad(1, much - 1 - i, False)
            return carry

        lax.fori_loop(much * piece // pieces, much * (piece + 1) // pieces, step, 0)

    def attend_far_send():
        @pl.when(light)
        def _():
            far[...] = packed(acc_ref.at[1]).astype(jnp.bfloat16)
            answer.start()

    quads = e // 4

    def attend_first():
        attend_quad(0, quads, True)

    def attend(late, early, pieces):
        much = quads - jnp.where(heavy, shared, 0)
        lo, hi = jnp.where(heavy, late[0], early[0]), jnp.where(heavy, late[1], early[1])

        def step(i, carry):
            attend_quad(0, quads - i, False)
            return carry

        lax.fori_loop(1 + much * lo // pieces, 1 + much * hi // pieces, step, 0)

    aw = apart.shape[1]
    ar = [
        rc(apart.at[to], aland.at[i], ats.at[i], atr.at[i], (e, to)) for i, to in enumerate((right, left, opp))
    ]

    def project():
        attended_ref[...] = packed(acc_ref.at[0])

        @pl.when(heavy)
        def _():
            answer.wait_recv()
            attended_ref[...] += jnp.exp2(-packed(near_ref.at[0])) * landed[...].astype(jnp.float32)

        attended = attended_ref[...].astype(jnp.bfloat16)
        step = 512
        for s in range(0, wo.shape[1], step):
            value = jnp.dot(attended, wo[:, s : s + step], preferred_element_type=jnp.float32)
            apart[:, :, s : s + step] = value.reshape(4, aw, step).astype(jnp.bfloat16)
        for copy in ar:
            copy.start()

    def project_last():
        total = apart[t].astype(jnp.float32)
        for i, copy in enumerate(ar):
            copy.wait_recv()
            total = total + aland[i].astype(jnp.float32)
        att_out[...] = total.astype(jnp.bfloat16)

    def returned():
        all_back = rc(ret.at[1:], ret.at[1:], rts.at[0], rtr, (e, t))
        all_back.wait_recv()
        own_back.wait()

    def combine():
        back_rows = flat(ret).astype(jnp.bfloat16)
        total = None
        for k in range(2):
            got = jnp.dot(pick[k], back_rows, preferred_element_type=jnp.float32) * scale[:, 2 + k : 3 + k]
            total = got if total is None else total + got
        exp_out[...] = total.astype(jnp.bfloat16)

    dispatch(1, 0, 2)
    kv_round(1)
    dispatch(1, 2, 3)
    kv_round(2)
    dispatch(2)
    dispatch(0)
    kv_round(3)
    spread_rows(1)
    dispatch(3)
    ask_partner()
    kv_first()
    spread_rows(2)
    forward_rows(1)
    loads_ready()
    experts(0)
    spread_rows(3)
    kv_second()
    experts(1)
    forward_rows(2)
    forward_hidden(0)
    kv_third()
    weights_ready()
    forward_rows(3)
    kv_ready()
    attend_far_start()
    attend_far(0, 2)
    attend_first()
    forward_hidden(1)
    attend((0, 1), (0, 0), 4)
    experts(2)
    attend_far(1, 2)
    attend_far_send()
    attend((1, 2), (0, 0), 4)
    give_back(1)
    experts(3)
    give_back(0)
    forward_hidden(2)
    attend((2, 3), (0, 1), 4)
    forward_hidden(3)
    give_back(2)
    attend((3, 4), (1, 4), 4)
    give_back(3)
    project()
    returned()
    combine()
    project_last()

    for g in range(groups):
        arrived(g).wait_send()
        ref = res.at[g, 1 if g == 0 else 0 : count[g]]
        rc(ref, ref, rts.at[g], rtr, (e, t)).wait_send()
        for copy in ags_all[g] + hgs_all[g]:
            copy.wait_send()
    @pl.when(heavy)
    def _():
        ask.wait_send()

    @pl.when(light)
    def _():
        answer.wait_send()

    for copy in kz[0] + kz[1] + kx + kc + ar + wsend:
        copy.wait_send()


def body(
    query_rows, key_rows, retrieved_vector_table, key_bias, score_offset, out_weight, second_batch_activations,
    norm_gain, expert_index, route_weight, gate_weight, up_weight, down_weight,
):
    ne = lax.axis_size("ep")
    tokens, width = second_batch_activations.shape
    wide = width // 4
    groups = len(DISTANCES)
    most = max(len(d) for d in DISTANCES) * NX * NC
    many = max(len(d) for d in DISTANCES[1:]) * NX * NC
    heads = query_rows.shape[1] // HD
    bf, f32 = jnp.bfloat16, jnp.float32
    vmem, dma = pltpu.VMEM, pltpu.SemaphoreType.DMA
    vspec, aspec = pl.BlockSpec(memory_space=pltpu.VMEM), pl.BlockSpec(memory_space=pl.ANY)
    aw = tokens // 4
    return pl.pallas_call(
        whole_kernel,
        out_shape=(
            jax.ShapeDtypeStruct((aw, width), bf),
            jax.ShapeDtypeStruct((tokens, wide), bf),
        ),
        in_specs=[pl.BlockSpec(memory_space=pltpu.SMEM)] + [vspec] * 8 + [aspec] * 4,
        out_specs=(vspec, vspec),
        scratch_shapes=[
            vmem((NX * NC, ne // (NX * NC), ROWS + 16, ROWS), bf),
            vmem((2, heads * ROWS, 2 * ROWS), bf),
            vmem((2 * ROWS, 2 * ROWS), bf),
            vmem((2, heads * ROWS, ROWS), f32),
            vmem((2, heads * ROWS, ROWS), f32),
            vmem((ROWS, heads * HD), bf),
            vmem((ROWS, heads * HD), bf),
            vmem((ROWS, heads * HD), bf),
            vmem((ROWS, heads * HD), f32),
            vmem(gate_weight.shape[1:], bf),
            vmem(up_weight.shape[1:], bf),
            vmem((4 * down_weight.shape[1], wide), bf),
            vmem(out_weight.shape, bf),
            vmem((ne, CAP, width), bf),
            vmem((2, tokens, ne * CAP), bf),
            vmem((tokens, tokens), f32),
            vmem((len(DISTANCES[0]) * NX * NC, CAP, width), bf),
            vmem((4, groups - 1, many, CAP, wide), bf),
            vmem((4, groups, most * CAP, gate_weight.shape[2]), bf),
            vmem((groups, most, CAP, wide), bf),
            vmem((ne, CAP, wide), bf),
            vmem((4, aw, width), bf),
            vmem((3, aw, width), bf),
            dma((4,)), dma((3,)), dma((2, 4)), dma((2, 4)), dma((4,)), dma((4,)), dma((4,)), dma((4,)),
            dma((groups,)), dma((groups,)), dma((4, groups)), dma((4, groups)), dma((4, groups)), dma((4, groups)), dma((3,)), dma((3,)),
            dma((groups,)), dma, dma((3,)), dma((3,)), dma((2,)), dma((2,)),
        ],
        compiler_params=pltpu.CompilerParams(
            collective_id=0, has_side_effects=True, vmem_limit_bytes=56 * 1024 * 1024
        ),
    )(
        score_offset, key_rows.T, retrieved_vector_table.T, key_bias.T, query_rows, second_batch_activations,
        norm_gain.reshape(1, width), expert_index.T, route_weight.T, gate_weight[0], up_weight[0], down_weight[0],
        out_weight,
    )


def solution(mesh):
    return jax.shard_map(
        body,
        mesh=mesh,
        in_specs=(
            P("ep", "tp"),
            P("ep", "tp"),
            P("ep", "tp"),
            P("ep", "tp"),
            P("tp"),
            P("tp", None),
            P("ep", None),
            P(),
            P("ep", None),
            P("ep", None),
            P("ep", None, "tp"),
            P("ep", None, "tp"),
            P("ep", "tp", None),
        ),
        out_specs=(P(("ep", "tp"), None), P("ep", "tp")),
        check_vma=False,
    )
```

```python
import jax
import jax.numpy as jnp
from jax import lax
from jax.experimental import pallas as pl
from jax.experimental.pallas import tpu as pltpu
from jax.sharding import PartitionSpec as P

HD = 64
LOG2E = 1.4426950408889634
ROWS = 128


def dot_rows(a, b):
    return lax.dot_general(a, b, (((1,), (1,)), ((), ())), preferred_element_type=jnp.float32)


def block_update(lhs, off, pairs, tri, near, masks):
    dots = [
        jnp.dot(lhs, jnp.concatenate([kv, kv], axis=0), preferred_element_type=jnp.float32) for kv, _ in pairs
    ]
    logs, sums, heads_of = [], [], []
    for n, (d, (_, bias)) in enumerate(zip(dots, pairs)):
        s = jnp.concatenate(
            [d[h * ROWS : (h + 1) * ROWS] + (bias - off[h]) for h in range(len(off))], axis=0
        )
        soft = jnp.maximum(s, jnp.log2(1.0 + jnp.exp2(jnp.minimum(s, 126.0))))
        logw = s - soft
        if masks is not None:
            row = lax.broadcasted_iota(jnp.int32, s.shape, 0) % ROWS + masks[n]
            later = row > lax.broadcasted_iota(jnp.int32, s.shape, 1)
            soft = jnp.where(later, soft, 0.0)
            logw = jnp.where(later, logw, -jnp.inf)
        logs.append(logw)
        heads_of.append(soft[:, :1])
        sums.append(jnp.dot(soft.astype(jnp.bfloat16), tri, preferred_element_type=jnp.float32))
    out = None
    for logw, total, first, (kv, _) in zip(logs, sums, heads_of, pairs):
        value = dot_rows(jnp.exp2(logw - total).astype(jnp.bfloat16), kv)
        if near is not None:
            value = value * jnp.exp2(-near)
        out = value if out is None else out + value
        step = jnp.broadcast_to(total[:, :1] + first, (total.shape[0], ROWS))
        near = step if near is None else near + step
    return out, near


def query_lhs(q):
    q2 = q.astype(jnp.float32) * (0.125 * LOG2E)
    hi = q2.astype(jnp.bfloat16)
    lo = (q2 - hi.astype(jnp.float32)).astype(jnp.bfloat16)
    zero = jnp.zeros((ROWS, HD), jnp.bfloat16)
    parts = []
    for h in range(q.shape[1] // HD):
        cut = slice(h * HD, (h + 1) * HD)
        parts.append(jnp.concatenate([hi[:, cut], zero, lo[:, cut], zero], axis=1))
    return jnp.concatenate(parts, axis=0)


def triangle():
    r = lax.broadcasted_iota(jnp.int32, (2 * ROWS, 2 * ROWS), 0)
    c = lax.broadcasted_iota(jnp.int32, (2 * ROWS, 2 * ROWS), 1)
    return jnp.where(r > c, 1.0, 0.0).astype(jnp.bfloat16)


NX, NC, CAP = 4, 2, 8
DISTANCES = ((0,), (3, 5, 4), (2, 6), (1, 7))
MESH = pl.DeviceIdType.MESH


def whole_kernel(
    off_ref, kt_ref, vt_ref, bias_ref, q_ref, act_ref, gain_ref, idxt_ref, routet_ref, wg_hbm, wu_hbm, wd_hbm, wo_hbm,
    att_out, exp_out,
    kvb, lhs_ref, tri_ref, acc_ref, near_ref, qfar, far, landed, attended_ref,
    wg, wu, wd, wo,
    outgoing, pick, scale, direct, arr, hid, res, ret,
    apart, aland,
    wsem, lsem, kzs, kzr, kxs, kxr, kcs, kcr, ds, dr, ags, agr, hgs, hgr, wds, wdr, rts, rtr, ats, atr, qss, qsr,
):
    e, t = lax.axis_index("ep"), lax.axis_index("tp")
    nz = lax.axis_size("ep") // (NX * NC)
    ne = nz * NX * NC
    tokens = act_ref.shape[0]
    heads = q_ref.shape[1] // HD
    groups = len(DISTANCES)
    count = [len(d) * NX * NC for d in DISTANCES]
    wide = arr.shape[-1]
    z, x, c = e // (NX * NC), e // NC % NX, e % NC
    xc = x * NC + c
    left, right, opp = (t + 3) % 4, (t + 1) % 4, (t + 2) % 4

    def ep_of(z_, x_, c_):
        return (z_ * NX + x_) * NC + c_

    def rc(src, dst, ssem, rsem, dev):
        return pltpu.make_async_remote_copy(
            src_ref=src, dst_ref=dst, send_sem=ssem, recv_sem=rsem, device_id=dev, device_id_type=MESH
        )

    barrier = pltpu.get_barrier_semaphore()

    def greet(i, carry):
        pl.semaphore_signal(barrier, inc=1, device_id=((e + i) % ne, t), device_id_type=MESH)
        return carry

    lax.fori_loop(1, ne, greet, 0, unroll=True)
    for near_t in (left, right, opp):
        pl.semaphore_signal(barrier, inc=1, device_id=(e, near_t), device_id_type=MESH)

    ff = wd_hbm.shape[0]

    def columns(to):
        return wd_hbm.at[:, pl.ds(pl.multiple_of(to * wide, wide), wide)]

    def part_rows(of):
        return wd.at[pl.ds(pl.multiple_of(of * ff, ff), ff)]

    loads = [
        pltpu.make_async_copy(src, dst, wsem.at[i])
        for i, (src, dst) in enumerate(((wg_hbm, wg), (wu_hbm, wu), (columns(t), part_rows(t)), (wo_hbm, wo)))
    ]
    for load in loads:
        load.start()
    kvb[xc, z] = jnp.concatenate(
        [kt_ref[...], vt_ref[...], jnp.broadcast_to(bias_ref[...].astype(jnp.float32), (16, ROWS)).astype(jnp.bfloat16)],
        axis=0,
    )

    pl.semaphore_wait(barrier, ne + 2)

    zr, zl = (ep_of((z + 1) % nz, x, c), t), (ep_of((z + nz - 1) % nz, x, c), t)

    def round_z(way, step):
        if way == 0:
            i, dev = (z + nz - step) % nz, zr
        else:
            i, dev = (z + step) % nz, zl
        return rc(kvb.at[xc, i], kvb.at[xc, i], kzs.at[way, step], kzr.at[way, step], dev)

    steps_z = (nz // 2, nz - 1 - nz // 2)
    kz = [[round_z(way, step) for step in range(steps_z[way])] for way in range(2)]

    def kv_round(step):
        for way in range(2):
            if 0 < step <= steps_z[way]:
                kz[way][step - 1].wait_recv()
            if step < steps_z[way]:
                kz[way][step].start()

    kv_round(0)

    at_right, at_left = (e, right), (e, left)
    wsend = [
        rc(columns(to), part_rows(t), wds.at[i], wdr.at[i], (e, to)) for i, to in enumerate((right, left, opp))
    ]

    def weights_ready():
        for copy in wsend:
            copy.wait_recv()
        for load in loads[2:]:
            load.wait()

    def loads_ready():
        for load in loads[:2]:
            load.wait()

    for copy in wsend:
        copy.start()

    values = act_ref[...].astype(jnp.float32)
    inv = lax.rsqrt(jnp.mean(values * values, axis=1, keepdims=True) + 1e-06)
    mine = pl.ds(pl.multiple_of(t * wide, wide), wide)
    i0 = lax.broadcasted_iota(jnp.int32, (tokens, tokens), 0)
    i1 = lax.broadcasted_iota(jnp.int32, (tokens, tokens), 1)
    below = jnp.where(i0 > i1, 1.0, 0.0).astype(jnp.bfloat16)
    above = jnp.where(i0 < i1, 1.0, 0.0).astype(jnp.bfloat16)
    idxt = [idxt_ref[k : k + 1, :] for k in range(2)]
    index = jnp.concatenate([idxt_ref[...].astype(jnp.float32), routet_ref[...], jnp.zeros((tokens - 4, tokens), jnp.float32)], axis=0).T
    scale[...] = index
    eq = [jnp.where(i1.astype(jnp.float32) == index[:, k : k + 1], 1.0, 0.0) for k in range(2)]
    prefix = jnp.dot(below, (eq[0] + eq[1]).astype(jnp.bfloat16), preferred_element_type=jnp.float32)
    eqt = [jnp.where(i0 == idxt[k], 1.0, 0.0) for k in range(2)]
    prefixt = jnp.dot((eqt[0] + eqt[1]).astype(jnp.bfloat16), above, preferred_element_type=jnp.float32)
    slots = ne * CAP
    col = lax.broadcasted_iota(jnp.int32, (tokens, slots), 1).astype(jnp.float32)
    row = lax.broadcasted_iota(jnp.int32, (slots, tokens), 0).astype(jnp.float32)
    spread = None
    for k in range(2):
        place = jnp.sum(eq[k] * prefix, axis=1, keepdims=True) + index[:, k : k + 1] * CAP
        pick[k] = jnp.where(col == place, 1.0, 0.0).astype(jnp.bfloat16)
        placet = jnp.sum(eqt[k] * prefixt, axis=0, keepdims=True) + idxt[k].astype(jnp.float32) * CAP
        one = jnp.where(row == placet, 1.0, 0.0)
        spread = one if spread is None else spread + one
    spread = spread.astype(jnp.bfloat16)
    for s in range(0, act_ref.shape[1], wide):
        cols = slice(s, s + wide)
        normed = (act_ref[:, cols].astype(jnp.float32) * inv * gain_ref[:, cols]).astype(jnp.bfloat16)
        sent = jnp.dot(spread, normed, preferred_element_type=jnp.float32)
        outgoing[:, :, cols] = sent.reshape(ne, CAP, wide).astype(jnp.bfloat16)
    lhs_ref[0] = query_lhs(q_ref[...])
    acc_ref[1] = jnp.zeros(acc_ref.shape[1:], jnp.float32)
    near_ref[1] = jnp.zeros(near_ref.shape[1:], jnp.float32)
    tri_ref[...] = triangle()
    off = [off_ref[h] * LOG2E for h in range(heads)]

    def peer(g, i, sign):
        per = NX * NC
        dz = DISTANCES[g][-1] % nz
        for n in range(len(DISTANCES[g]) - 1, 0, -1):
            dz = jnp.where(i < n * per, DISTANCES[g][n - 1] % nz, dz)
        dx, dc = i // NC % NX, i % NC
        if sign < 0:
            dz, dx = nz - dz, NX - dx
        return ep_of((z + dz) % nz, (x + dx) % NX, (c + dc) % NC)

    own_rows = pltpu.make_async_copy(outgoing.at[e], direct.at[0], lsem.at[1])
    own_rows.start()
    def dispatch(g, first=0, last=3):
        def scatter(i, carry):
            to = peer(g, i, 1)
            if g == 0:
                src, dst = outgoing.at[to], direct.at[i]
            else:
                src, dst = outgoing.at[to, :, mine], arr.at[t, g - 1, i]
            rc(src, dst, ds.at[g], dr.at[g], (to, t)).start()
            return carry

        per = NX * NC
        lax.fori_loop(1 if g == 0 else first * per, min(last * per, count[g]), scatter, 0)

    def arrived(g):
        ref = direct.at[1:] if g == 0 else arr.at[t, g - 1, : count[g]]
        return rc(ref, ref, ds.at[g], dr.at[g], (e, t))

    def ag(g):
        n, half = count[g], count[g] // 2
        a, left_rows, right_rows = arr.at[t, g - 1, :n], arr.at[left, g - 1, :half], arr.at[right, g - 1, half:n]
        return [
            rc(a, a, ags.at[0, g], agr.at[0, g], at_right),
            rc(a, a, ags.at[1, g], agr.at[1, g], at_left),
            rc(left_rows, left_rows, ags.at[2, g], agr.at[2, g], at_right),
            rc(right_rows, right_rows, ags.at[3, g], agr.at[3, g], at_left),
        ]

    ags_all = [[]] + [ag(g) for g in range(1, groups)]

    def spread_rows(g):
        arrived(g).wait_recv()
        ags_all[g][0].start()
        ags_all[g][1].start()

    def forward_rows(g):
        ags_all[g][0].wait_recv()
        ags_all[g][2].start()
        ags_all[g][1].wait_recv()
        ags_all[g][3].start()

    xl, xr, xo = (x + 3) % NX, (x + 1) % NX, (x + 2) % NX
    dev_xr, dev_xl, dev_c = (ep_of(z, xr, c), t), (ep_of(z, xl, c), t), (ep_of(z, x, (c + 1) % NC), t)
    zh = nz // 2

    def grp(x_):
        return kvb.at[x_ * NC + c]

    kx = [
        rc(grp(x), grp(x), kxs.at[0], kxr.at[0], dev_xr),
        rc(grp(x), grp(x), kxs.at[1], kxr.at[1], dev_xl),
        rc(kvb.at[xl * NC + c, :zh], kvb.at[xl * NC + c, :zh], kxs.at[2], kxr.at[2], dev_xr),
        rc(kvb.at[xr * NC + c, zh:], kvb.at[xr * NC + c, zh:], kxs.at[3], kxr.at[3], dev_xl),
    ]
    kc = [rc(grp(x_), grp(x_), kcs.at[i], kcr.at[i], dev_c) for i, x_ in enumerate((x, xl, xr, xo))]

    def kv_first():
        kv_round(4)
        kx[0].start()
        kx[1].start()
        kc[0].start()

    def kv_second():
        kx[0].wait_recv()
        kx[2].start()
        kc[1].start()
        kx[1].wait_recv()
        kx[3].start()
        kc[2].start()

    def kv_third():
        kx[2].wait_recv()
        kx[3].wait_recv()
        kc[3].start()

    def kv_ready():
        for copy in kc:
            copy.wait_recv()


    def flat(ref):
        v = ref[...].astype(jnp.float32)
        return v.reshape(v.shape[0] * v.shape[1], v.shape[2])

    def experts(g):
        if g == 0:
            arrived(0).wait_recv()
            own_rows.wait()
            xs = flat(direct).astype(jnp.bfloat16)
        else:
            ags_all[g][2].wait_recv()
            ags_all[g][3].wait_recv()
            xs = jnp.concatenate([flat(arr.at[s, g - 1, : count[g]]).astype(jnp.bfloat16) for s in range(4)], axis=1)
        gate = jnp.dot(xs, wg[...], preferred_element_type=jnp.float32)
        up = jnp.dot(xs, wu[...], preferred_element_type=jnp.float32)
        hidden = (gate / (1.0 + jnp.exp(-gate)) * up).astype(jnp.bfloat16)
        hid[t, g, : count[g] * CAP] = hidden
        hgs_all[g][0].start()
        hgs_all[g][1].start()

    def hg(g):
        rows, half = count[g] * CAP, count[g] * CAP // 2
        a, left_rows, right_rows = hid.at[t, g, :rows], hid.at[left, g, :half], hid.at[right, g, half:rows]
        return [
            rc(a, a, hgs.at[0, g], hgr.at[0, g], at_right),
            rc(a, a, hgs.at[1, g], hgr.at[1, g], at_left),
            rc(left_rows, left_rows, hgs.at[2, g], hgr.at[2, g], at_right),
            rc(right_rows, right_rows, hgs.at[3, g], hgr.at[3, g], at_left),
        ]

    hgs_all = [hg(g) for g in range(groups)]

    def forward_hidden(g):
        hgs_all[g][0].wait_recv()
        hgs_all[g][2].start()
        hgs_all[g][1].wait_recv()
        hgs_all[g][3].start()

    own_back = pltpu.make_async_copy(res.at[0, 0], ret.at[e], lsem.at[2])

    def give_back(g):
        hgs_all[g][2].wait_recv()
        hgs_all[g][3].wait_recv()
        hidden = jnp.concatenate([hid[s, g, : count[g] * CAP] for s in range(4)], axis=1)
        value = jnp.dot(hidden, wd[...], preferred_element_type=jnp.float32)
        res[g, : count[g]] = value.reshape(count[g], CAP, wide).astype(jnp.bfloat16)
        if g == 0:
            own_back.start()

        def back(i, carry):
            to = peer(g, i, -1)
            rc(res.at[g, i], ret.at[e], rts.at[g], rtr, (to, t)).start()
            return carry

        lax.fori_loop(1 if g == 0 else 0, count[g], back, 0)

    def load_pair(b):
        i, j = b % (NX * NC), b // (NX * NC)
        kv = jnp.concatenate([kvb[i, j, :ROWS], kvb[i + 1, j, :ROWS]], axis=1)
        bias = jnp.concatenate([kvb[i, j, ROWS:][:1], kvb[i + 1, j, ROWS:][:1]], axis=1)
        return kv, bias.astype(jnp.float32) * LOG2E

    heavy, light = z >= nz // 2, z < nz // 2
    shared = jnp.where(heavy, 2 * z + 1 - nz, nz - 1 - 2 * z) * (NX * NC // 8)
    partner = (ep_of(nz - 1 - z, x, c), t)
    ask = rc(q_ref, qfar, qss.at[0], qsr.at[0], partner)
    answer = rc(far, landed, qss.at[1], qsr.at[1], partner)

    def attend_quad(slot, quad, first):
        pairs = [load_pair(quad * 4 + 2), load_pair(quad * 4)]
        own = e % 4 * ROWS
        lhs, tri = lhs_ref[slot], tri_ref[...]
        near = None if first else near_ref[slot]
        result = block_update(lhs, off, pairs, tri, near, (own - 2 * ROWS, own) if first else None)
        acc_ref[slot] = result[0] if first else acc_ref[slot] + result[0]
        near_ref[slot] = result[1]

    def packed(ref):
        lane = lax.broadcasted_iota(jnp.int32, (ROWS, ROWS), 1)
        pairs = []
        for h in range(0, heads, 2):
            even = pltpu.roll(ref[h * ROWS : (h + 1) * ROWS, :], HD, 1)
            odd = ref[(h + 1) * ROWS : (h + 2) * ROWS, :]
            pairs.append(jnp.where(lane < HD, even, odd))
        return jnp.concatenate(pairs, axis=1)

    def ask_partner():
        @pl.when(heavy)
        def _():
            ask.start()

    def attend_far_start():
        @pl.when(light)
        def _():
            ask.wait_recv()
            lhs_ref[1] = query_lhs(qfar[...])

    def attend_far(piece, pieces):
        much = jnp.where(light, shared, 0)

        def step(i, carry):
            attend_quad(1, much - 1 - i, False)
            return carry

        lax.fori_loop(much * piece // pieces, much * (piece + 1) // pieces, step, 0)

    def attend_far_send():
        @pl.when(light)
        def _():
            far[...] = packed(acc_ref.at[1]).astype(jnp.bfloat16)
            answer.start()

    quads = e // 4

    def attend_first():
        attend_quad(0, quads, True)

    def attend(late, early, pieces):
        much = quads - jnp.where(heavy, shared, 0)
        lo, hi = jnp.where(heavy, late[0], early[0]), jnp.where(heavy, late[1], early[1])

        def step(i, carry):
            attend_quad(0, quads - i, False)
            return carry

        lax.fori_loop(1 + much * lo // pieces, 1 + much * hi // pieces, step, 0)

    aw = apart.shape[1]
    ar = [
        rc(apart.at[to], aland.at[i], ats.at[i], atr.at[i], (e, to)) for i, to in enumerate((right, left, opp))
    ]

    def project():
        attended_ref[...] = packed(acc_ref.at[0])

        @pl.when(heavy)
        def _():
            answer.wait_recv()
            attended_ref[...] += jnp.exp2(-packed(near_ref.at[0])) * landed[...].astype(jnp.float32)

        attended = attended_ref[...].astype(jnp.bfloat16)
        step = 512
        for s in range(0, wo.shape[1], step):
            value = jnp.dot(attended, wo[:, s : s + step], preferred_element_type=jnp.float32)
            apart[:, :, s : s + step] = value.reshape(4, aw, step).astype(jnp.bfloat16)
        for copy in ar:
            copy.start()

    def project_last():
        total = apart[t].astype(jnp.float32)
        for i, copy in enumerate(ar):
            copy.wait_recv()
            total = total + aland[i].astype(jnp.float32)
        att_out[...] = total.astype(jnp.bfloat16)

    def returned():
        all_back = rc(ret.at[1:], ret.at[1:], rts.at[0], rtr, (e, t))
        all_back.wait_recv()
        own_back.wait()

    def combine():
        back_rows = flat(ret).astype(jnp.bfloat16)
        total = None
        for k in range(2):
            got = jnp.dot(pick[k], back_rows, preferred_element_type=jnp.float32) * scale[:, 2 + k : 3 + k]
            total = got if total is None else total + got
        exp_out[...] = total.astype(jnp.bfloat16)

    dispatch(1, 0, 2)
    kv_round(1)
    dispatch(1, 2, 3)
    kv_round(2)
    dispatch(2)
    dispatch(0)
    kv_round(3)
    spread_rows(1)
    dispatch(3)
    ask_partner()
    kv_first()
    spread_rows(2)
    forward_rows(1)
    loads_ready()
    experts(0)
    spread_rows(3)
    kv_second()
    experts(1)
    forward_rows(2)
    forward_hidden(0)
    kv_third()
    weights_ready()
    forward_rows(3)
    kv_ready()
    attend_far_start()
    attend_far(0, 2)
    attend_first()
    forward_hidden(1)
    attend((0, 1), (0, 0), 4)
    experts(2)
    attend_far(1, 2)
    attend_far_send()
    attend((1, 2), (0, 0), 4)
    give_back(1)
    experts(3)
    give_back(0)
    forward_hidden(2)
    attend((2, 3), (0, 1), 4)
    forward_hidden(3)
    give_back(2)
    attend((3, 4), (1, 4), 4)
    give_back(3)
    project()
    returned()
    combine()
    project_last()

    for g in range(groups):
        arrived(g).wait_send()
        ref = res.at[g, 1 if g == 0 else 0 : count[g]]
        rc(ref, ref, rts.at[g], rtr, (e, t)).wait_send()
        for copy in ags_all[g] + hgs_all[g]:
            copy.wait_send()
    @pl.when(heavy)
    def _():
        ask.wait_send()

    @pl.when(light)
    def _():
        answer.wait_send()

    for copy in kz[0] + kz[1] + kx + kc + ar + wsend:
        copy.wait_send()


def body(
    query_rows, key_rows, retrieved_vector_table, key_bias, score_offset, out_weight, second_batch_activations,
    norm_gain, expert_index, route_weight, gate_weight, up_weight, down_weight,
):
    ne = lax.axis_size("ep")
    tokens, width = second_batch_activations.shape
    wide = width // 4
    groups = len(DISTANCES)
    most = max(len(d) for d in DISTANCES) * NX * NC
    many = max(len(d) for d in DISTANCES[1:]) * NX * NC
    heads = query_rows.shape[1] // HD
    bf, f32 = jnp.bfloat16, jnp.float32
    vmem, dma = pltpu.VMEM, pltpu.SemaphoreType.DMA
    vspec, aspec = pl.BlockSpec(memory_space=pltpu.VMEM), pl.BlockSpec(memory_space=pl.ANY)
    aw = tokens // 4
    return pl.pallas_call(
        whole_kernel,
        out_shape=(
            jax.ShapeDtypeStruct((aw, width), bf),
            jax.ShapeDtypeStruct((tokens, wide), bf),
        ),
        in_specs=[pl.BlockSpec(memory_space=pltpu.SMEM)] + [vspec] * 8 + [aspec] * 4,
        out_specs=(vspec, vspec),
        scratch_shapes=[
            vmem((NX * NC, ne // (NX * NC), ROWS + 16, ROWS), bf),
            vmem((2, heads * ROWS, 2 * ROWS), bf),
            vmem((2 * ROWS, 2 * ROWS), bf),
            vmem((2, heads * ROWS, ROWS), f32),
            vmem((2, heads * ROWS, ROWS), f32),
            vmem((ROWS, heads * HD), bf),
            vmem((ROWS, heads * HD), bf),
            vmem((ROWS, heads * HD), bf),
            vmem((ROWS, heads * HD), f32),
            vmem(gate_weight.shape[1:], bf),
            vmem(up_weight.shape[1:], bf),
            vmem((4 * down_weight.shape[1], wide), bf),
            vmem(out_weight.shape, bf),
            vmem((ne, CAP, width), bf),
            vmem((2, tokens, ne * CAP), bf),
            vmem((tokens, tokens), f32),
            vmem((len(DISTANCES[0]) * NX * NC, CAP, width), bf),
            vmem((4, groups - 1, many, CAP, wide), bf),
            vmem((4, groups, most * CAP, gate_weight.shape[2]), bf),
            vmem((groups, most, CAP, wide), bf),
            vmem((ne, CAP, wide), bf),
            vmem((4, aw, width), bf),
            vmem((3, aw, width), bf),
            dma((4,)), dma((3,)), dma((2, 4)), dma((2, 4)), dma((4,)), dma((4,)), dma((4,)), dma((4,)),
            dma((groups,)), dma((groups,)), dma((4, groups)), dma((4, groups)), dma((4, groups)), dma((4, groups)), dma((3,)), dma((3,)),
            dma((groups,)), dma, dma((3,)), dma((3,)), dma((2,)), dma((2,)),
        ],
        compiler_params=pltpu.CompilerParams(
            collective_id=0, has_side_effects=True, vmem_limit_bytes=56 * 1024 * 1024
        ),
    )(
        score_offset, key_rows.T, retrieved_vector_table.T, key_bias.T, query_rows, second_batch_activations,
        norm_gain.reshape(1, width), expert_index.T, route_weight.T, gate_weight[0], up_weight[0], down_weight[0],
        out_weight,
    )


def solution(mesh):
    return jax.shard_map(
        body,
        mesh=mesh,
        in_specs=(
            P("ep", "tp"),
            P("ep", "tp"),
            P("ep", "tp"),
            P("ep", "tp"),
            P("tp"),
            P("tp", None),
            P("ep", None),
            P(),
            P("ep", None),
            P("ep", None),
            P("ep", None, "tp"),
            P("ep", None, "tp"),
            P("ep", "tp", None),
        ),
        out_specs=(P(("ep", "tp"), None), P("ep", "tp")),
        check_vma=False,
    )
```
